32 devices in a mesh: grp: 2 (over y), sp: 4 (over z), tp: 4 (over x, core).
Axes of the slice: x: 2, y: 2, z: 4, core: 2. Of those that a mesh axis runs over, the one named last changes fastest.
Arguments:
- query_a: bfloat16 [3072, 1024], P(('grp', 'sp'), 'tp'), parts along dimension 0, may hold values from -6 to 6
- key_a: bfloat16 [3072, 1024], P(('grp', 'sp'), 'tp'), parts along dimension 0, may hold values from -6 to 6
- query_b: bfloat16 [3072, 512], P(('grp', 'sp'), 'tp'), parts along dimension 0, may hold values from -6 to 6
- key_b: bfloat16 [3072, 512], P(('grp', 'sp'), 'tp'), parts along dimension 0, may hold values from -6 to 6
- values_a: bfloat16 [3072, 2048], P(('grp', 'sp'), 'tp'), parts along dimension 0, may hold values from -6 to 6
- values_b: bfloat16 [3072, 2048], P(('grp', 'sp'), 'tp'), parts along dimension 0, may hold values from -6 to 6
- outgate_a: bfloat16 [3072, 2048], P(('grp', 'sp'), 'tp'), parts along dimension 0, may hold values from -8 to 8
- outgate_b: bfloat16 [3072, 2048], P(('grp', 'sp'), 'tp'), parts along dimension 0, may hold values from -8 to 8
- input_pre: float32 [2, 8, 3072], P(None, 'tp', ('grp', 'sp')), parts along dimension 2, may hold values from -8 to 110, as said below
- forget_pre: float32 [2, 8, 3072], P(None, 'tp', ('grp', 'sp')), parts along dimension 2, may hold values from -4 to 16
- resid: bfloat16 [3072, 2048], P(('grp', 'sp', 'tp')), parts along dimension 0, may hold values from -6 to 6
- out_proj: bfloat16 [2048, 2, 2048], P(None, None, 'tp'), may hold values from -0.1875 to 0.1875
- norm_gain: float32 [2048], replicated, may hold values from 0.1 to 1.9
- w_gate: bfloat16 [2048, 5120], P('sp', 'tp'), may hold values from -0.125 to 0.125
- w_up: bfloat16 [2048, 5120], P('sp', 'tp'), may hold values from -0.125 to 0.125
- w_down: bfloat16 [2048, 5120], P('sp', 'tp'), may hold values from -0.078125 to 0.078125
Outputs:
- mixed: bfloat16 [3072, 2048], P(('grp', 'sp', 'tp')), parts along dimension 0
The draws below stay inside these ranges and needn't reach their ends.
There are 2 independent parts, one for each index of `grp`. The reference program is written for one: setup_inputs(seed, part) draws one part's arguments, and reference() takes and returns one part's arrays. A program takes and returns all parts, laid end to end along the dimension named above; an argument that names none is the same for every part. Nothing has to cross between parts.
Inputs may be any that keep to these rules, and one draw needn't show every extreme that they name: `input_pre`: pre-activations of the exponential input gate.
All inputs are finite; a program needn't handle non-finite values.
Results may differ from the reference program's by a relative error of at most 0.014.
Values may be sent and summed in bfloat16 or wider, within the bound.
A program may use at most 64 MiB of HBM per device.

```python
import math
import jax
import jax.numpy as jnp
from jax import lax

D = 2048
FF = 5120
GROUP_HEADS = 8
DKA = 128
DKB = 64
DV = 256
TOK_DEV = 384
SEQUENCE_LENGTH = 1536
N_TP = 4


def draw_input_pre(key, part):
    complete_shape = (2, GROUP_HEADS, SEQUENCE_LENGTH)
    value_rows = 1.2 * jax.random.normal(jax.random.fold_in(key, 16), complete_shape, jnp.float32)
    return jnp.clip(value_rows, -8.0, 110.0)


def draw_forget_pre(key, part):
    complete_shape = (2, GROUP_HEADS, SEQUENCE_LENGTH)
    block_count = SEQUENCE_LENGTH // TOK_DEV
    fast_share = 0.5
    quick_head = jax.random.uniform(jax.random.fold_in(key, 21), (2, GROUP_HEADS, 1), jnp.float32) < fast_share
    keep_ratio = jnp.exp(jax.random.uniform(jax.random.fold_in(key, 22), (2, GROUP_HEADS, 1), jnp.float32, math.log(0.15), math.log(0.7)))
    slow_base = jnp.log(SEQUENCE_LENGTH / keep_ratio)
    fast_base = jax.random.uniform(jax.random.fold_in(key, 23), (2, GROUP_HEADS, 1), jnp.float32, 2.5, 4.0)
    offsets = jax.random.uniform(jax.random.fold_in(key, 24), (2, GROUP_HEADS, block_count, 1), jnp.float32, -0.7, 0.7)
    offsets = jnp.broadcast_to(offsets, (2, GROUP_HEADS, block_count, TOK_DEV)).reshape(complete_shape)
    jitter = jnp.clip(0.6 * jax.random.normal(jax.random.fold_in(key, 26), complete_shape, jnp.float32), -1.8, 1.8)
    spike_entries = jax.random.randint(jax.random.fold_in(key, 27), (2, GROUP_HEADS, 2, 1), 0, SEQUENCE_LENGTH)
    spike_position = jnp.any(jnp.arange(SEQUENCE_LENGTH)[None, None, None, :] == spike_entries, axis=2)
    spike_magnitude = jax.random.uniform(jax.random.fold_in(key, 28), complete_shape, jnp.float32, 0.0, 1.4)
    value_rows = jnp.where(quick_head, fast_base, slow_base) + offsets + jitter
    value_rows = jnp.where(jnp.logical_and(spike_position, jnp.logical_not(quick_head)), spike_magnitude, value_rows)
    return jnp.clip(value_rows, -4.0, 16.0)


def steps_of(stream_key, dims, pieces, least, top_value):
    gain = 1.0
    for dim, shards_of in pieces:
        steps = jax.random.uniform(jax.random.fold_in(jax.random.fold_in(stream_key, 6), dim), (shards_of,), jnp.float32, least / len(pieces), top_value / len(pieces))
        gain = gain * jnp.repeat(jnp.exp(steps), dims[dim] // shards_of).reshape((-1,) + (1,) * (len(dims) - 1 - dim))
    return gain


def noise(key, dims, scale, reach, shards=(), held_as=jnp.bfloat16):
    values = scale * jax.random.normal(key, dims, jnp.float32)
    if shards:
        values = values * steps_of(key, dims, shards, -0.22, 0.18)
    return jnp.clip(values, -reach, reach).astype(held_as)


def setup_inputs(seed: int = 0, part: int = 0) -> dict:
    key_of = jax.random.split(jax.random.key(seed), 17)
    part_splits = jax.random.split(jax.random.fold_in(key_of[16], part), 17)
    query_a = noise(part_splits[0], (SEQUENCE_LENGTH, GROUP_HEADS * DKA), 1.0, 6.0, ((0, 4), (1, 4)))
    key_a = noise(part_splits[1], (SEQUENCE_LENGTH, GROUP_HEADS * DKA), 1.0, 6.0, ((0, 4), (1, 4)))
    query_b = noise(part_splits[2], (SEQUENCE_LENGTH, GROUP_HEADS * DKB), 1.0, 6.0, ((0, 4), (1, 4)))
    key_b = noise(part_splits[3], (SEQUENCE_LENGTH, GROUP_HEADS * DKB), 1.0, 6.0, ((0, 4), (1, 4)))
    values_a = noise(part_splits[4], (SEQUENCE_LENGTH, GROUP_HEADS * DV), 1.0, 6.0, ((0, 4), (1, 4)))
    values_b = noise(part_splits[5], (SEQUENCE_LENGTH, GROUP_HEADS * DV), 1.0, 6.0, ((0, 4), (1, 4)))
    outgate_a = noise(part_splits[6], (SEQUENCE_LENGTH, GROUP_HEADS * DV), 1.5, 8.0, ((0, 4), (1, 4)))
    outgate_b = noise(part_splits[7], (SEQUENCE_LENGTH, GROUP_HEADS * DV), 1.5, 8.0, ((0, 4), (1, 4)))
    input_pre = draw_input_pre(jax.random.fold_in(jax.random.fold_in(key_of[16], part), 71), part)
    forget_pre = draw_forget_pre(jax.random.fold_in(jax.random.fold_in(key_of[16], part), 71), part)
    resid = noise(part_splits[10], (SEQUENCE_LENGTH, D), 1.0, 6.0, ((0, 16),))
    out_proj = noise(key_of[11], (D, 2, GROUP_HEADS * DV), (GROUP_HEADS * DV // 2) ** -0.5, 0.1875, ((2, 4),))
    norm_gain = jnp.clip(1.0 + 0.18 * jax.random.normal(key_of[12], (D,), jnp.float32), 0.1, 1.9)
    w_gate = noise(key_of[13], (D, FF), D ** -0.5, 0.125, ((0, 4), (1, 4)))
    w_up = noise(key_of[14], (D, FF), D ** -0.5, 0.125, ((0, 4), (1, 4)))
    w_down = noise(key_of[15], (D, FF), FF ** -0.5, 0.078125, ((0, 4), (1, 4)))
    return {"query_a": query_a, "key_a": key_a, "query_b": query_b, "key_b": key_b, "values_a": values_a, "values_b": values_b, "outgate_a": outgate_a, "outgate_b": outgate_b, "input_pre": input_pre, "forget_pre": forget_pre, "resid": resid, "out_proj": out_proj, "norm_gain": norm_gain, "w_gate": w_gate, "w_up": w_up, "w_down": w_down}


EPS = 1e-06
NEG = -1e+30

def summarize(key_heads, value_head_rows, input_log, forget_raw):
    cum_forget = jnp.cumsum(jax.nn.log_sigmoid(forget_raw), axis=1)
    offset_log = input_log - cum_forget
    block_sum = cum_forget[:, -1]
    block_max = block_sum + lax.optimization_barrier(jnp.max(offset_log, axis=1))
    key_decay = jnp.exp(block_sum[:, None] + offset_log - block_max[:, None])
    scaled_keys = (key_heads.astype(jnp.float32) * jnp.transpose(key_decay)[:, :, None]).astype(jnp.bfloat16)
    block_memory_state = jnp.einsum('eif,eiw->ifw', scaled_keys.astype(jnp.float32), value_head_rows.astype(jnp.float32))
    return (block_memory_state, block_max, block_sum, offset_log)

def head_outputs(query_head_rows, key_heads, value_head_rows, outgate, offset_log, carried_over, mstate, key_width):
    length = query_head_rows.shape[0]
    run_max = jnp.maximum(lax.cummax(offset_log, axis=1), mstate[:, None])
    causal = jnp.arange(length)[:, None] >= jnp.arange(length)[None, :]
    exponent = jnp.where(causal[None], offset_log[:, None, :] - run_max[:, :, None], -jnp.inf)
    scores = jnp.einsum('thk,shk->hts', query_head_rows.astype(jnp.float32), key_heads.astype(jnp.float32))
    scores = scores * key_width ** (-0.5) * jnp.exp(exponent)
    weights_bf = scores.astype(jnp.bfloat16)
    inner_part = jnp.einsum('hts,shv->thv', weights_bf.astype(jnp.float32), value_head_rows.astype(jnp.float32))
    carried_portion = jnp.einsum('pix,ixe->pie', query_head_rows.astype(jnp.float32), carried_over, precision=lax.Precision.HIGHEST) * key_width ** (-0.5)
    carried_portion = carried_portion * jnp.transpose(jnp.exp(mstate[:, None] - run_max))[:, :, None]
    numerator = carried_portion + inner_part
    inv_rms = lax.rsqrt(lax.optimization_barrier(jnp.mean(numerator * numerator, axis=2, keepdims=True)) + EPS)
    gated_out = numerator * inv_rms * jax.nn.sigmoid(outgate.astype(jnp.float32).reshape(numerator.shape))
    return gated_out.reshape(length, -1).astype(jnp.bfloat16)

def advance(earlier, later_part):
    state_one_a, state_one_b, max_one, sum_one = earlier
    state_two_a, state_two_b, max_two, sum_two = later_part
    merged_max = jnp.maximum(sum_two + max_one, max_two)
    keep_old = jnp.exp(sum_two + max_one - merged_max)
    keep_new = jnp.exp(max_two - merged_max)
    merged_a = keep_old[0][:, None, None] * state_one_a + keep_new[0][:, None, None] * state_two_a
    merged_b = keep_old[1][:, None, None] * state_one_b + keep_new[1][:, None, None] * state_two_b
    return (merged_a, merged_b, merged_max, sum_one + sum_two)

def reference(query_a, key_a, query_b, key_b, values_a, values_b, outgate_a, outgate_b, input_pre, forget_pre, resid, out_proj, norm_gain, w_gate, w_up, w_down):
    block_count = SEQUENCE_LENGTH // TOK_DEV

    def blocks(array, width):
        return array.reshape(block_count, TOK_DEV, GROUP_HEADS, width)

    def gate_blocks(array):
        return jnp.transpose(array.reshape(2, GROUP_HEADS, block_count, TOK_DEV), (2, 0, 1, 3))
    inputs = (blocks(query_a, DKA), blocks(key_a, DKA), blocks(query_b, DKB), blocks(key_b, DKB), blocks(values_a, DV), blocks(values_b, DV), outgate_a.reshape(block_count, TOK_DEV, GROUP_HEADS * DV), outgate_b.reshape(block_count, TOK_DEV, GROUP_HEADS * DV), gate_blocks(input_pre), gate_blocks(forget_pre))

    def advance_block(carry_all, block_in):
        query_ha, key_ha, query_hb, key_hb, value_ha, value_hb, gate_oa, gate_ob, input_blk, forget_blk = block_in
        state_a, max_a, sum_a, offset_a = summarize(key_ha, value_ha, input_blk[0], forget_blk[0])
        state_b, max_b, sum_b, offset_b = summarize(key_hb, value_hb, input_blk[1], forget_blk[1])
        hidden_a = head_outputs(query_ha, key_ha, value_ha, gate_oa, offset_a, carry_all[0], carry_all[2][0], DKA)
        hidden_b = head_outputs(query_hb, key_hb, value_hb, gate_ob, offset_b, carry_all[1], carry_all[2][1], DKB)
        updated = advance(carry_all, (state_a, state_b, jnp.stack([max_a, max_b]), jnp.stack([sum_a, sum_b])))
        return (updated, jnp.stack([hidden_a, hidden_b], axis=1))
    initial = (jnp.zeros((GROUP_HEADS, DKA, DV), jnp.float32), jnp.zeros((GROUP_HEADS, DKB, DV), jnp.float32), jnp.full((2, GROUP_HEADS), NEG, jnp.float32), jnp.zeros((2, GROUP_HEADS), jnp.float32))
    unused, hidden = lax.scan(advance_block, initial, inputs)
    set_width = GROUP_HEADS // N_TP * DV
    hidden = hidden.reshape(SEQUENCE_LENGTH, 2, N_TP, set_width)
    proj_sets = out_proj.reshape(D, 2, N_TP, set_width)
    attn_out = jnp.zeros((SEQUENCE_LENGTH, D), jnp.float32)
    for member in range(N_TP):
        hidden_set = hidden[:, :, member, :].reshape(SEQUENCE_LENGTH, 2 * set_width)
        weight_set = proj_sets[:, :, member, :].reshape(D, 2 * set_width)
        partial_value = jnp.dot(hidden_set, jnp.transpose(weight_set), preferred_element_type=jnp.float32)
        attn_out = attn_out + lax.optimization_barrier(partial_value.astype(jnp.bfloat16)).astype(jnp.float32)
    resid_sum = resid.astype(jnp.float32) + attn_out
    normed = resid_sum * lax.rsqrt(lax.optimization_barrier(jnp.mean(resid_sum * resid_sum, axis=1, keepdims=True)) + EPS) * norm_gain
    normed = normed.astype(jnp.bfloat16)
    gate_act = jnp.dot(normed, w_gate, preferred_element_type=jnp.float32)
    up_act = jnp.dot(normed, w_up, preferred_element_type=jnp.float32)
    inner_act = (jax.nn.silu(gate_act) * up_act).astype(jnp.bfloat16)
    unit_width = FF // N_TP
    ffn_out = jnp.zeros((SEQUENCE_LENGTH, D), jnp.float32)
    for member in range(N_TP):
        inner_cols = inner_act[:, member * unit_width:(member + 1) * unit_width]
        down_cols = w_down[:, member * unit_width:(member + 1) * unit_width]
        partial_value = jnp.dot(inner_cols, jnp.transpose(down_cols), preferred_element_type=jnp.float32)
        ffn_out = ffn_out + lax.optimization_barrier(partial_value.astype(jnp.bfloat16)).astype(jnp.float32)
    return (resid_sum + ffn_out).astype(jnp.bfloat16)
```

```python
import functools

import jax
import jax.numpy as jnp
from jax import lax
from jax.experimental import pallas as pl
from jax.experimental.pallas import tpu as pltpu
from jax.sharding import PartitionSpec as P

DKA = 128
DKB = 64
DV = 256


EPS = 1e-06
NEG = -1e30


def summarize(key_heads, value_head_rows, input_log, forget_raw):
    cum_forget = jnp.cumsum(jax.nn.log_sigmoid(forget_raw), axis=1)
    offset_log = input_log - cum_forget
    block_sum = cum_forget[:, -1]
    block_max = block_sum + jnp.max(offset_log, axis=1)
    key_decay = jnp.exp(block_sum[:, None] + offset_log - block_max[:, None])
    scaled_keys = (key_heads.astype(jnp.float32) * jnp.transpose(key_decay)[:, :, None]).astype(
        jnp.bfloat16
    )
    block_memory_state = jnp.einsum(
        "eif,eiw->ifw", scaled_keys, value_head_rows, preferred_element_type=jnp.float32
    )
    return (block_memory_state, block_max, block_sum, offset_log)


def head_outputs(
    query_head_rows,
    key_heads,
    value_head_rows,
    outgate,
    offset_log,
    carried_over,
    mstate,
    key_width,
):
    length = query_head_rows.shape[0]
    run_max = jnp.maximum(lax.cummax(offset_log, axis=1), mstate[:, None])
    causal = jnp.arange(length)[:, None] >= jnp.arange(length)[None, :]
    exponent = jnp.where(causal[None], offset_log[:, None, :] - run_max[:, :, None], -jnp.inf)
    scores = jnp.einsum(
        "thk,shk->hts", query_head_rows, key_heads, preferred_element_type=jnp.float32
    )
    scores = scores * key_width ** (-0.5) * jnp.exp(exponent)
    weights_bf = scores.astype(jnp.bfloat16)
    inner_part = jnp.einsum(
        "hts,shv->thv", weights_bf, value_head_rows, preferred_element_type=jnp.float32
    )
    carried_portion = jnp.einsum(
        "pix,ixe->pie",
        query_head_rows,
        carried_over.astype(jnp.bfloat16),
        preferred_element_type=jnp.float32,
    ) * key_width ** (-0.5)
    carried_portion = (
        carried_portion * jnp.transpose(jnp.exp(mstate[:, None] - run_max))[:, :, None]
    )
    numerator = carried_portion + inner_part
    inv_rms = lax.rsqrt(jnp.mean(numerator * numerator, axis=2, keepdims=True) + EPS)
    gated_out = (
        numerator * inv_rms * jax.nn.sigmoid(outgate.astype(jnp.float32).reshape(numerator.shape))
    )
    return gated_out.reshape(length, -1).astype(jnp.bfloat16)


def shifted(value, axis, shift):
    count = lax.axis_size(axis)
    return lax.ppermute(value, axis, [(i, (i + shift) % count) for i in range(count)])


def swapped(value, axis):
    count = lax.axis_size(axis)
    return lax.ppermute(value, axis, [(i, i ^ 1) for i in range(count)])


def side_swapped(value):
    return swapped(value, "grp")


def column_shifted(value, shift):
    count = lax.axis_size("tp")
    return lax.ppermute(value, "tp", [(i, (i + 2 * shift) % count) for i in range(count)])


def split_wide(value):
    high = lax.reduce_precision(value, 8, 7)
    middle = lax.reduce_precision(value - high, 8, 7)
    return jnp.stack([high, middle, value - high - middle]).astype(jnp.bfloat16)


def entering(state_a, state_b, stats):
    count, mine = lax.axis_size("sp"), lax.axis_index("sp")
    heads, depth_a, width = state_a.shape
    depth_b = state_b.shape[1]
    terms = split_wide(stats).transpose(3, 0, 1, 2).reshape(heads, 1, 12)
    terms = jnp.pad(terms, ((0, 0), (0, 15), (0, width - 12)))
    packed = jnp.concatenate(
        [state_a.astype(jnp.bfloat16), state_b.astype(jnp.bfloat16), terms], axis=1
    )
    parts = [
        lax.ppermute(packed, "sp", [(i, i + step) for i in range(count - step)])
        for step in range(1, count)
    ]
    total = jnp.zeros_like(stats[1])
    highest = jnp.full_like(stats[0], NEG)
    logs = []
    for step in range(1, count):
        got = parts[step - 1][:, depth_a + depth_b, :12].astype(jnp.float32)
        stat = jnp.sum(got.reshape(heads, 3, 2, 2), axis=1).transpose(1, 2, 0)
        logs.append(jnp.where(step <= mine, stat[0] + total, NEG))
        total = total + stat[1]
        highest = jnp.maximum(highest, logs[-1])
    carried_a, carried_b = jnp.zeros_like(state_a), jnp.zeros_like(state_b)
    for step in range(1, count):
        weight = jnp.where(step <= mine, jnp.exp(logs[step - 1] - highest), 0.0)[:, :, None, None]
        part = parts[step - 1].astype(jnp.float32)
        carried_a += weight[0] * part[:, :depth_a]
        carried_b += weight[1] * part[:, depth_a : depth_a + depth_b]
    return carried_a, carried_b, highest


def scatter_pair(partial):
    chips = lax.axis_size("tp") // 2
    me = lax.axis_index("tp")
    chip, core = me // 2, me % 2
    parts = partial.reshape(2, chips, 2, -1, partial.shape[-1])
    away = lax.dynamic_index_in_dim(parts, 1 - core, 2, keepdims=False).astype(jnp.bfloat16)
    kept = lax.dynamic_index_in_dim(parts, core, 2, keepdims=False)
    got = swapped(away, "tp")
    totals = []
    for which in (1, 0):
        both = kept[which].astype(jnp.float32) + got[which].astype(jnp.float32)
        total = lax.dynamic_index_in_dim(both, chip, 0, keepdims=False)
        for step in range(1, chips):
            target = lax.rem(chip + step, chips)
            sent = lax.dynamic_index_in_dim(both, target, 0, keepdims=False).astype(jnp.bfloat16)
            total = total + column_shifted(sent, step).astype(jnp.float32)
        totals.append(total)
    return totals[1] + swapped(totals[0].astype(jnp.bfloat16), "sp").astype(jnp.float32)


def scatter_rows(partial):
    chips = lax.axis_size("tp") // 2
    me = lax.axis_index("tp")
    chip, core = me // 2, me % 2
    parts = partial.reshape(chips, 2, -1, partial.shape[-1])
    away = lax.dynamic_index_in_dim(parts, 1 - core, 1, keepdims=False).astype(jnp.bfloat16)
    kept = lax.dynamic_index_in_dim(parts, core, 1, keepdims=False)
    both = kept.astype(jnp.float32) + swapped(away, "tp").astype(jnp.float32)
    total = lax.dynamic_index_in_dim(both, chip, 0, keepdims=False)
    for step in range(1, chips):
        target = lax.rem(chip + step, chips)
        sent = lax.dynamic_index_in_dim(both, target, 0, keepdims=False).astype(jnp.bfloat16)
        total = total + column_shifted(sent, step).astype(jnp.float32)
    return total


def gather_rows(rows):
    chips = lax.axis_size("tp") // 2
    core = lax.axis_index("tp") % 2
    mine = jnp.stack([rows] + [column_shifted(rows, step) for step in range(1, chips)])
    other = swapped(mine, "tp")
    first = jnp.where(core == 0, mine, other)
    second = jnp.where(core == 0, other, mine)
    gathered = jnp.stack([first, second], axis=1)
    return gathered.reshape(-1, rows.shape[-1])


def by_owner(partial):
    chips = lax.axis_size("tp") // 2
    chip = lax.axis_index("tp") // 2
    parts = partial.reshape(chips, -1, partial.shape[-1])
    order = [
        lax.dynamic_index_in_dim(parts, lax.rem(chip - owner + chips, chips), 0)
        for owner in range(chips)
    ]
    return jnp.concatenate(order).reshape(partial.shape)


def local(
    query_a,
    key_a,
    query_b,
    key_b,
    values_a,
    values_b,
    outgate_a,
    outgate_b,
    input_pre,
    forget_pre,
    resid,
    out_proj,
    norm_gain,
    w_gate,
    w_up,
    w_down,
):
    tokens_dev = query_a.shape[0]
    heads_dev = query_a.shape[1] // DKA
    count, place, part = lax.axis_size("sp"), lax.axis_index("sp"), lax.axis_index("grp")
    depth, units = w_gate.shape
    half = units // 2
    side = lax.rem(place, 2)

    def columns(weight, step):
        target_side = lax.rem(place + step, 2)
        return lax.dynamic_slice_in_dim(weight, target_side * half, half, 1)

    lead = jnp.where(part == 0, w_gate, w_up)
    first_sent = columns(lead, 1)
    lead_parts = [None, shifted(first_sent, "sp", 1)]
    key_heads_a = key_a.reshape(tokens_dev, heads_dev, DKA)
    key_heads_b = key_b.reshape(tokens_dev, heads_dev, DKB)
    value_heads_a = values_a.reshape(tokens_dev, heads_dev, DV)
    value_heads_b = values_b.reshape(tokens_dev, heads_dev, DV)
    state_a, max_a, sum_a, offset_a = summarize(
        key_heads_a, value_heads_a, input_pre[0], forget_pre[0]
    )
    state_b, max_b, sum_b, offset_b = summarize(
        key_heads_b, value_heads_b, input_pre[1], forget_pre[1]
    )
    stats = jnp.stack([jnp.stack([max_a, max_b]), jnp.stack([sum_a, sum_b])])
    lead, w_down, state_a, state_b, stats = lax.optimization_barrier(
        (lead, w_down, state_a, state_b, stats)
    )
    carried_a, carried_b, mstate = entering(state_a, state_b, stats)
    for step in range(2, count):
        lead_parts.append(shifted(columns(lead, step), "sp", step))
    down_mine = lax.dynamic_slice_in_dim(w_down, part * (depth // 2), depth // 2, 0)
    down_parts = [None] + [
        shifted(columns(down_mine, step), "sp", step) for step in range(1, count)
    ]
    hidden_a = head_outputs(
        query_a.reshape(tokens_dev, heads_dev, DKA),
        key_heads_a,
        value_heads_a,
        outgate_a,
        offset_a,
        carried_a,
        mstate[0],
        DKA,
    )
    hidden_b = head_outputs(
        query_b.reshape(tokens_dev, heads_dev, DKB),
        key_heads_b,
        value_heads_b,
        outgate_b,
        offset_b,
        carried_b,
        mstate[1],
        DKB,
    )
    hidden = jnp.stack([hidden_a, hidden_b], axis=1).reshape(tokens_dev, -1)
    proj_weight = out_proj.reshape(out_proj.shape[0], -1)
    row_block = hidden
    attn_rows = scatter_rows(
        lax.dot_general(
            row_block, proj_weight, (((1,), (1,)), ((), ())), preferred_element_type=jnp.float32
        )
    )
    resid_sum = resid.astype(jnp.float32) + attn_rows
    normed = (
        resid_sum
        * lax.rsqrt(jnp.mean(resid_sum * resid_sum, axis=1, keepdims=True) + EPS)
        * norm_gain
    )
    normed = normed.astype(jnp.bfloat16)
    pair_normed = swapped(normed, "sp")
    own = lambda weight: lax.dynamic_slice_in_dim(weight, side * half, half, 1)
    own_trail = jnp.where(part == 0, own(w_up), own(w_gate))
    lead_parts[0] = own(lead)
    trail_parts = [own_trail] + [side_swapped(piece) for piece in lead_parts[1:]]
    other_down = lax.dynamic_slice_in_dim(w_down, (1 - part) * (depth // 2), depth // 2, 0)
    down_parts[0] = own(down_mine)
    down_other = [own(other_down)] + [side_swapped(piece) for piece in down_parts[1:]]

    def placed(pieces, offset, blocks):
        whole = jnp.zeros((blocks * depth, half), jnp.bfloat16)
        for step, (first, second) in enumerate(pieces):
            origin = lax.rem(place - step + count, count) * depth
            whole = lax.dynamic_update_slice_in_dim(whole, first, origin + part * offset, 0)
            if second is not None:
                whole = lax.dynamic_update_slice_in_dim(
                    whole, second, origin + (1 - part) * offset, 0
                )
        return whole

    lead_full = placed([(piece, None) for piece in lead_parts], 0, count)
    trail_full = placed([(piece, None) for piece in trail_parts], 0, count)
    down_full = placed(list(zip(down_parts, down_other)), depth // 2, count)
    rows = jnp.concatenate([gather_rows(normed), gather_rows(pair_normed)])
    lead_act = jnp.dot(rows, lead_full, preferred_element_type=jnp.float32)
    trail_act = jnp.dot(rows, trail_full, preferred_element_type=jnp.float32)
    gate_act = jnp.where(part == 0, lead_act, trail_act)
    up_act = jnp.where(part == 0, trail_act, lead_act)
    inner_act = (jax.nn.silu(gate_act) * up_act).astype(jnp.bfloat16)
    partial = lax.dot_general(
        inner_act, down_full, (((1,), (1,)), ((), ())), preferred_element_type=jnp.float32
    ).astype(jnp.bfloat16)
    partial = partial.reshape(2, -1, partial.shape[-1])
    partial = jnp.stack([by_owner(partial[0]), by_owner(partial[1])])
    return (resid_sum + scatter_pair(partial)).astype(jnp.bfloat16)


MESH = pl.DeviceIdType.MESH
NT = (((1,), (1,)), ((), ()))
TN = (((0,), (0,)), ((), ()))
F32 = jnp.float32
BF16 = jnp.bfloat16
SUBS = 2
LAG_B, LAG_C, LAG_D, RING = 2, 5, 8, 8
VMEM_BYTES = 60 * 2**20


def scan_lanes(value, combine, neutral):
    length = value.shape[1]
    lane = lax.broadcasted_iota(jnp.int32, value.shape, 1)
    step = 1
    while step < length:
        moved = jnp.where(lane >= step, pltpu.roll(value, step, 1), neutral)
        value = combine(value, moved)
        step *= 2
    return value


def fused_body(
    sizes,
    query_a,
    key_a,
    query_b,
    key_b,
    values_a,
    values_b,
    outgate_a,
    outgate_b,
    input_pre,
    forget_pre,
    resid,
    out_proj,
    gain,
    w_gate,
    w_up,
    w_down,
    out_ref,
    qa, ka, qb, kb, va, vb, oga, ogb, inp, fgt, res, proj, gn,
    wg, wu, wd,
    cols, offs, bstate, st_out, st_in, stat_out, stat_in, intra, hidden,
    part1, keep1, dsend1, drecv1, xsend1, xrecv1, rsum,
    rows, act, inner, part2, keep2, dsend2, drecv2, xsend2, xrecv2, zsend2, zrecv2,
    lsem, zs, zr, ys, yr, cs, cr, d1s, d1r, x1s, x1r, ags, agr,
    d2s, d2r, x2s, x2r, z2s, z2r,
):
    count, tokens, heads, depth, half, block, chunk1, _ = sizes
    g, s, t = lax.axis_index("grp"), lax.axis_index("sp"), lax.axis_index("tp")
    x, c = lax.div(t, 2), lax.rem(t, 2)
    core_peer = (g, s, t + 1 - 2 * c)
    x_peer = (g, s, t + 2 - 4 * x)
    y_peer = (1 - g, s, t)
    pair = (g, s + 1 - 2 * lax.rem(s, 2), t)
    part_rows = depth // 2
    sub_rows = part_rows // SUBS

    def remote(src, dst, send, recv, device):
        return pltpu.make_async_remote_copy(
            src_ref=src, dst_ref=dst, send_sem=send, recv_sem=recv,
            device_id=device, device_id_type=MESH,
        )

    barrier = pltpu.get_barrier_semaphore()
    for device in (core_peer, x_peer, y_peer):
        pl.semaphore_signal(barrier, inc=1, device_id=device, device_id_type=MESH)
    for place in range(count):
        @pl.when(place != s)
        def _():
            pl.semaphore_signal(barrier, inc=1, device_id=(g, place, t), device_id_type=MESH)

    side = lax.rem(s, 2)
    own_cols = pl.ds(pl.multiple_of(side * half, 128), half)
    own_rows = pl.ds(pl.multiple_of(s * depth, depth), depth)
    loads = [
        (input_pre, inp), (forget_pre, fgt), (key_a, ka), (key_b, kb), (values_a, va),
        (values_b, vb), (query_a, qa), (query_b, qb), (outgate_a, oga), (outgate_b, ogb),
        (out_proj, proj), (resid, res), (gain, gn),
        (w_gate.at[:, own_cols], wg.at[own_rows]),
        (w_up.at[:, own_cols], wu.at[own_rows]),
        (w_down.at[:, own_cols], wd.at[own_rows]),
    ]
    local = [pltpu.make_async_copy(a, b, lsem.at[i]) for i, (a, b) in enumerate(loads)]
    for copy in local:
        copy.start()

    whole_of = (wg, wu) + (wd,) * SUBS
    held_of = (w_gate, w_up) + (w_down,) * SUBS

    def piece_rows(pid, source, which):
        if pid < 2:
            return pl.ds(pl.multiple_of(source * depth + which * part_rows, part_rows), part_rows)
        start = source * depth + which * part_rows + (pid - 2) * sub_rows
        return pl.ds(pl.multiple_of(start, sub_rows), sub_rows)

    def z_copy(pid, dest):
        start = g * part_rows + (0 if pid < 2 else (pid - 2) * sub_rows)
        size = part_rows if pid < 2 else sub_rows
        src = held_of[pid].at[
            pl.ds(pl.multiple_of(start, sub_rows), size), pl.ds((dest % 2) * half, half)
        ]
        return remote(
            src, whole_of[pid].at[piece_rows(pid, s, g)],
            zs.at[pid, dest], zr.at[pid, s], (g, dest, t),
        )

    def y_copy(pid, source, which):
        place = whole_of[pid].at[piece_rows(pid, source, which)]
        return remote(place, place, ys.at[pid, source], yr.at[pid, source], y_peer)

    def arrived_z(pid, source):
        place = whole_of[pid].at[piece_rows(pid, source, g)]
        remote(place, place, zs.at[pid, source], zr.at[pid, source], y_peer).wait_recv()

    def issue(pids, want):
        for pid in pids:
            for dest in list(range(count)):
                @pl.when(jnp.logical_and(dest < s, want(dest)))
                def _():
                    z_copy(pid, dest).start()
            for dest in reversed(range(count)):
                @pl.when(jnp.logical_and(dest > s, want(dest)))
                def _():
                    z_copy(pid, dest).start()

    last = count - 1
    at_end = jnp.logical_or(s == 0, s == last)

    def far(dest):
        return jnp.logical_or(jnp.logical_not(at_end), jnp.abs(dest - s) == last)

    def near(dest):
        return jnp.logical_not(far(dest))

    def source_at(step):
        up_room, down_room = last - s, s
        small = jnp.minimum(up_room, down_room)
        both = jnp.where(step % 2 == 1, s + (step + 1) // 2, s - step // 2)
        beyond = jnp.where(up_room > down_room, s + step - small, s - step + small)
        return jnp.where(step <= 2 * small, both, beyond)

    def forward(pid, step):
        source = source_at(step)
        arrived_z(pid, source)
        y_copy(pid, source, g).start()

    pl.semaphore_wait(barrier, 3 + count - 1)
    issue((0,), lambda dest: dest < s)
    issue((1,), lambda dest: jnp.logical_and(dest < s, far(dest)))
    issue((0,), lambda dest: dest > s)

    for i in range(2):
        local[i].wait()
    quad = lambda ref: jnp.concatenate([ref[0], ref[1], ref[0], ref[1]], axis=0)
    raw_forget, raw_input = quad(fgt), quad(inp)
    log_forget = jnp.minimum(raw_forget, 0.0) - jnp.log1p(jnp.exp(-jnp.abs(raw_forget)))
    cum = scan_lanes(log_forget, lambda a, b: a + b, 0.0)
    offset = raw_input - cum
    run = scan_lanes(offset, jnp.maximum, NEG)
    fsum = cum[:, tokens - 1 : tokens]
    top = run[:, tokens - 1 : tokens]
    bmax = fsum + top
    decay = jnp.exp(offset - top)
    offs[...] = offset
    group = 2 * heads
    cols[...] = jnp.transpose(jnp.concatenate([decay[:group], run[:group]], axis=0))

    for i in range(2, 6):
        local[i].wait()
    head_lane = lax.div(lax.broadcasted_iota(jnp.int32, (tokens, heads * DKB), 1), DKB)
    state_of = []
    for h in range(heads):
        column = cols[:, h : h + 1]
        scaled = (ka[:, h * DKA : (h + 1) * DKA].astype(F32) * column).astype(BF16)
        state = lax.dot_general(
            scaled, va[:, h * DV : (h + 1) * DV], TN, preferred_element_type=F32
        )
        bstate[h * DKA : (h + 1) * DKA, :] = state
        state_of.append((h * DKA, DKA, h))
    base_b = heads * DKA
    for h in range(heads):
        column = cols[:, heads + h : heads + h + 1]
        scaled = (kb[...].astype(F32) * column).astype(BF16)
        state = lax.dot_general(
            scaled, vb[:, h * DV : (h + 1) * DV], TN, preferred_element_type=F32
        )
        bstate[base_b + h * DKB : base_b + (h + 1) * DKB, :] = state[h * DKB : (h + 1) * DKB]
        state_of.append((base_b + h * DKB, DKB, heads + h))

    chain = [
        remote(st_out, st_in, cs.at[0], cr.at[0], (g, jnp.minimum(s + 1, last), t)),
        remote(stat_out, stat_in, cs.at[1], cr.at[1], (g, jnp.minimum(s + 1, last), t)),
    ]

    def combine_and_send():
        before = stat_in[...]
        total = before + fsum
        after = jnp.maximum(total, bmax)
        keep_old = jnp.exp(total - after)
        keep_new = jnp.exp(jnp.broadcast_to(bmax, total.shape) - after)
        stat_out[...] = after
        wide = lambda row: jnp.concatenate([row] * (DV // 128), axis=1)
        for start, size, h in state_of:
            old = wide(keep_old[h : h + 1, :])
            new = wide(keep_new[h : h + 1, :])
            st_out[start : start + size, :] = (
                old * st_in[start : start + size, :].astype(F32)
                + new * bstate[start : start + size, :]
            ).astype(BF16)
        for copy in chain:
            copy.start()

    @pl.when(s == 0)
    def _():
        st_in[...] = jnp.zeros_like(st_in)
        stat_in[...] = jnp.full_like(stat_in, NEG)
        combine_and_send()
        issue((1,), lambda dest: jnp.logical_and(dest > s, far(dest)))

    for i in range(6, 8):
        local[i].wait()
    causal = lax.broadcasted_iota(jnp.int32, (tokens, tokens), 0) >= lax.broadcasted_iota(
        jnp.int32, (tokens, tokens), 1
    )

    def query_of(h):
        if h < heads:
            return qa[:, h * DKA : (h + 1) * DKA]
        return jnp.where(head_lane == h - heads, qb[...], jnp.zeros_like(qb[...]))

    for h in range(group):
        key = ka[:, h * DKA : (h + 1) * DKA] if h < heads else kb[...]
        value_ref, at = (va, h) if h < heads else (vb, h - heads)
        width = DKA if h < heads else DKB
        scores = lax.dot_general(query_of(h), key, NT, preferred_element_type=F32)
        exponent = jnp.where(causal, offs[h : h + 1, :] - cols[:, group + h : group + h + 1], NEG)
        weights = (scores * width ** (-0.5) * jnp.exp(exponent)).astype(BF16)
        intra[h] = jnp.dot(
            weights, value_ref[:, at * DV : (at + 1) * DV], preferred_element_type=F32
        )

    @pl.when(s > 0)
    def _():
        for copy in chain:
            copy.wait_recv()

    @pl.when(jnp.logical_and(s > 0, s < last))
    def _():
        combine_and_send()
        issue((1,), lambda dest: jnp.logical_and(dest > s, far(dest)))

    for i in range(8, 10):
        local[i].wait()
    for h in range(group):
        width = DKA if h < heads else DKB
        gate_ref, at = (oga, h) if h < heads else (ogb, h - heads)
        state = (
            st_in[h * DKA : (h + 1) * DKA, :] if h < heads else st_in[base_b:, :]
        )
        entering_max = stat_in[h : h + 1, 0:1]
        own_max = cols[:, group + h : group + h + 1]
        top_max = jnp.maximum(own_max, entering_max)
        carried = jnp.dot(query_of(h), state, preferred_element_type=F32)
        numer = carried * (width ** (-0.5) * jnp.exp(entering_max - top_max)) + intra[
            h
        ] * jnp.exp(own_max - top_max)
        inv = lax.rsqrt(jnp.mean(numer * numer, axis=1, keepdims=True) + EPS)
        gated = numer * inv * jax.nn.sigmoid(gate_ref[:, at * DV : (at + 1) * DV].astype(F32))
        hidden[:, h * DV : (h + 1) * DV] = gated.astype(BF16)

    forward(0, 1)

    for i in range(10, 13):
        local[i].wait()
    chunks1 = proj.shape[0] // chunk1

    def block_rows(chip, core):
        return pl.ds(pl.multiple_of((2 * chip + core) * block, 8), block)

    def d1(j):
        return remote(dsend1.at[j], drecv1.at[j], d1s.at[j], d1r.at[j], core_peer)

    def x1(j):
        return remote(xsend1.at[j], xrecv1.at[j], x1s.at[j], x1r.at[j], x_peer)

    def attn_step(j, carry):
        @pl.when(j < chunks1)
        def _():
            weight = proj[pl.ds(pl.multiple_of(j * chunk1, chunk1), chunk1)]
            part1[...] = lax.dot_general(
                hidden[...], weight.reshape(chunk1, hidden.shape[1]), NT,
                preferred_element_type=F32,
            )
            for role in range(2):
                chip = x if role == 0 else 1 - x
                dsend1[j, role] = part1[block_rows(chip, 1 - c)].astype(BF16)
                keep1[j, role] = part1[block_rows(chip, c)]
            d1(j).start()

        @pl.when(j >= 1)
        def _():
            k = j - 1
            d1(k).wait_recv()
            xsend1[k] = (keep1[k, 1] + drecv1[k, 1].astype(F32)).astype(BF16)
            x1(k).start()
            keep1[k, 0] = keep1[k, 0] + drecv1[k, 0].astype(F32)

        return carry

    lax.fori_loop(0, chunks1 + 1, attn_step, 0)
    forward(0, 2)
    for j in range(chunks1):
        span = slice(j * chunk1, (j + 1) * chunk1)
        x1(j).wait_recv()
        rsum[:, span] = res[:, span].astype(F32) + keep1[j, 0] + xrecv1[j].astype(F32)
    summed = rsum[...]
    scale = lax.rsqrt(jnp.mean(summed * summed, axis=1, keepdims=True) + EPS)
    mine = block_rows(x, c)
    rows[0, mine] = (summed * scale * gn[...]).astype(BF16)

    def move(kind, src_place, dst_place, chip, core, device):
        return remote(
            rows.at[src_place, block_rows(chip, core)],
            rows.at[dst_place, block_rows(chip, core)],
            ags.at[kind], agr.at[kind], device,
        )

    own_z = move(2, 0, 1, x, c, pair)
    own_x = move(1, 0, 0, x, c, x_peer)
    own_d = move(0, 0, 0, x, c, core_peer)
    own_z.start()
    own_x.start()
    own_d.start()
    issue((1,), near)
    issue(range(2, 2 + SUBS), lambda dest: dest != s)

    def arrived(kind, place, chip, core):
        move(kind, place, place, chip, core, core_peer).wait_recv()

    forward(0, 3)
    arrived(1, 0, 1 - x, c)
    fwd_x = move(3, 0, 0, 1 - x, c, core_peer)
    fwd_x.start()
    forward(1, 1)
    arrived(2, 1, x, c)
    fwd_zx = move(5, 1, 1, x, c, x_peer)
    fwd_zd = move(4, 1, 1, x, c, core_peer)
    fwd_zx.start()
    fwd_zd.start()

    def arrived_y(pid, source):
        y_copy(pid, source, 1 - g).wait_recv()

    for i in range(13, 16):
        local[i].wait()
    for step in range(1, count):
        arrived_y(0, source_at(step))
    arrived(0, 0, x, 1 - c)
    arrived(3, 0, 1 - x, 1 - c)
    act[0] = jnp.dot(rows[0], wg[...], preferred_element_type=F32)
    arrived(5, 1, 1 - x, c)
    fwd_xd = move(6, 1, 1, 1 - x, c, core_peer)
    fwd_xd.start()
    forward(1, 2)
    forward(1, 3)
    arrived(4, 1, x, 1 - c)
    arrived(6, 1, 1 - x, 1 - c)
    act[1] = jnp.dot(rows[1], wg[...], preferred_element_type=F32)
    for step in range(1, count):
        arrived_y(1, source_at(step))

    def up_step(p, carry):
        gate = act[p]
        up = jnp.dot(rows[p], wu[...], preferred_element_type=F32)
        start = pl.multiple_of(p * tokens, tokens)
        inner[pl.ds(start, tokens), :] = (gate / (1.0 + jnp.exp(-gate)) * up).astype(BF16)
        return carry

    lax.fori_loop(0, 2, up_step, 0)

    rounds = count * SUBS
    chunks2 = 2 * rounds
    base = 2 * lax.div(s, 2)

    def place_of(p):
        is_y = jnp.logical_or(
            jnp.logical_and(p > 0, lax.rem(p, 2) == 0), p == chunks2 - 1
        )
        last_one = p == chunks2 - 1
        r = jnp.where(
            last_one, rounds - 1,
            jnp.where(is_y, lax.div(p, 2) - 1, lax.div(p + 1, 2)),
        )
        r = jnp.maximum(r, 0)
        span = 2 * SUBS
        b = lax.rem(base + lax.div(r, span) * 2 + lax.rem(r, 2), count)
        sub = lax.rem(lax.div(r, 2), SUBS)
        which = jnp.where(is_y, 1 - g, g)
        return b, sub, which, is_y

    def down_rows(p):
        b, sub, which, _ = place_of(p)
        return b * depth + which * part_rows + sub * sub_rows

    def d2(k):
        return remote(dsend2.at[k], drecv2.at[k], d2s.at[k], d2r.at[k], core_peer)

    def x2(k):
        return remote(xsend2.at[k], xrecv2.at[k], x2s.at[k], x2r.at[k], x_peer)

    def z2(k):
        return remote(zsend2.at[k], zrecv2.at[k], z2s.at[k], z2r.at[k], pair)

    def down_step(p, carry):
        @pl.when(p < chunks2)
        def _():
            b, sub, _, is_y = place_of(p)
            start = pl.multiple_of(down_rows(p), sub_rows)
            spot = wd.at[pl.ds(start, sub_rows)]
            pid = 2 + sub
            z_in = remote(spot, spot, zs.at[pid, b], zr.at[pid, b], y_peer)
            y_both = remote(spot, spot, ys.at[pid, b], yr.at[pid, b], y_peer)

            @pl.when(jnp.logical_and(b != s, jnp.logical_not(is_y)))
            def _():
                z_in.wait_recv()
                y_both.start()

            @pl.when(jnp.logical_and(b != s, is_y))
            def _():
                y_both.wait_recv()

            part2[...] = lax.dot_general(
                inner[...], wd[pl.ds(start, sub_rows), :], NT, preferred_element_type=F32
            )
            ring = lax.rem(p, RING)
            for place in range(2):
                for role in range(2):
                    chip = x if role == 0 else 1 - x
                    send = pl.multiple_of(place * tokens + (2 * chip + 1 - c) * block, 8)
                    hold = pl.multiple_of(place * tokens + (2 * chip + c) * block, 8)
                    dsend2[p, 2 * place + role] = part2[pl.ds(send, block)].astype(BF16)
                    keep2[ring, 2 * place + role] = part2[pl.ds(hold, block)]
            d2(p).start()

        @pl.when(jnp.logical_and(p >= LAG_B, p < chunks2 + LAG_B))
        def _():
            k = p - LAG_B
            ring = lax.rem(k, RING)
            d2(k).wait_recv()
            for place in range(2):
                xsend2[k, place] = (
                    keep2[ring, 2 * place + 1] + drecv2[k, 2 * place + 1].astype(F32)
                ).astype(BF16)
            x2(k).start()
            for place in range(2):
                keep2[ring, 2 * place] = keep2[ring, 2 * place] + drecv2[
                    k, 2 * place
                ].astype(F32)

        @pl.when(jnp.logical_and(p >= LAG_C, p < chunks2 + LAG_C))
        def _():
            k = p - LAG_C
            ring = lax.rem(k, RING)
            x2(k).wait_recv()
            zsend2[k] = (keep2[ring, 2] + xrecv2[k, 1].astype(F32)).astype(BF16)
            z2(k).start()
            span = pl.ds(pl.multiple_of(down_rows(k), sub_rows), sub_rows)
            rsum[:, span] = rsum[:, span] + keep2[ring, 0] + xrecv2[k, 0].astype(F32)

        @pl.when(p >= LAG_D)
        def _():
            k = p - LAG_D
            z2(k).wait_recv()
            span = pl.ds(pl.multiple_of(down_rows(k), sub_rows), sub_rows)
            out_ref[:, span] = (rsum[:, span] + zrecv2[k].astype(F32)).astype(BF16)

        return carry

    lax.fori_loop(0, chunks2 + LAG_D, down_step, 0)

    for pid in range(2 + SUBS):
        for dest in range(count):
            @pl.when(dest != s)
            def _():
                z_copy(pid, dest).wait_send()
                y_copy(pid, dest, g).wait_send()

    @pl.when(s < last)
    def _():
        for copy in chain:
            copy.wait_send()

    for copy in (own_z, own_x, own_d, fwd_x, fwd_zx, fwd_zd, fwd_xd):
        copy.wait_send()
    for j in range(chunks1):
        d1(j).wait_send()
        x1(j).wait_send()

    def drain(k, carry):
        d2(k).wait_send()
        x2(k).wait_send()
        z2(k).wait_send()
        return carry

    lax.fori_loop(0, chunks2, drain, 0)


def fused(*args):
    query_a, _, _, _, _ = args[:5]
    resid, w_gate = args[10], args[13]
    count = lax.axis_size("sp")
    tokens = query_a.shape[0]
    heads = query_a.shape[1] // DKA
    depth, units = w_gate.shape
    half = units // 2
    block, width = resid.shape
    chunk1 = width // 4
    chunk2 = depth // 2 // SUBS
    chunks1, chunks2 = width // chunk1, width // chunk2
    group = 2 * heads
    state_rows = heads * (DKA + DKB)
    sizes = (count, tokens, heads, depth, half, block, chunk1, chunk2)
    args = list(args)
    args[12] = args[12].reshape(1, width)
    vmem = lambda *shape, kind=BF16: pltpu.VMEM(shape, kind)
    dma = pltpu.SemaphoreType.DMA
    pieces = (2 + SUBS, count)
    copies = [args[i] for i in (0, 1, 2, 3, 4, 5, 6, 7, 8, 9, 10, 11, 12)]
    scratch = [pltpu.VMEM(a.shape, a.dtype) for a in copies]
    scratch += [vmem(width, half), vmem(width, half), vmem(width, half)]
    scratch += [
        vmem(tokens, 2 * group, kind=F32),
        vmem(2 * group, tokens, kind=F32),
        vmem(state_rows, DV, kind=F32),
        vmem(state_rows, DV),
        vmem(state_rows, DV),
        vmem(2 * group, 128, kind=F32),
        vmem(2 * group, 128, kind=F32),
        vmem(group, tokens, DV, kind=F32),
        vmem(tokens, group * DV),
        vmem(tokens, chunk1, kind=F32),
        vmem(chunks1, 2, block, chunk1, kind=F32),
        vmem(chunks1, 2, block, chunk1),
        vmem(chunks1, 2, block, chunk1),
        vmem(chunks1, block, chunk1),
        vmem(chunks1, block, chunk1),
        vmem(block, width, kind=F32),
        vmem(2, tokens, width),
        vmem(2, tokens, half, kind=F32),
        vmem(2 * tokens, half),
        vmem(2 * tokens, chunk2, kind=F32),
        vmem(RING, 4, block, chunk2, kind=F32),
        vmem(chunks2, 4, block, chunk2),
        vmem(chunks2, 4, block, chunk2),
        vmem(chunks2, 2, block, chunk2),
        vmem(chunks2, 2, block, chunk2),
        vmem(chunks2, block, chunk2),
        vmem(chunks2, block, chunk2),
    ]
    scratch += [dma((16,)), dma(pieces), dma(pieces), dma(pieces), dma(pieces), dma((2,)), dma((2,))]
    scratch += [dma((chunks1,))] * 4 + [dma((7,))] * 2 + [dma((chunks2,))] * 6
    return pl.pallas_call(
        functools.partial(fused_body, sizes),
        out_shape=jax.ShapeDtypeStruct(resid.shape, BF16),
        in_specs=[pl.BlockSpec(memory_space=pl.ANY)] * len(args),
        out_specs=pl.BlockSpec(memory_space=pltpu.VMEM),
        scratch_shapes=scratch,
        compiler_params=pltpu.CompilerParams(
            collective_id=0, has_side_effects=True, vmem_limit_bytes=VMEM_BYTES
        ),
    )(*args)


def layer(*args):
    return local(*args)


def solution(mesh):
    few = mesh.shape["sp"] == 4 and mesh.shape["tp"] == 4
    return jax.shard_map(
        fused if few else layer,
        mesh=mesh,
        in_specs=(
            P(("grp", "sp"), "tp"),
            P(("grp", "sp"), "tp"),
            P(("grp", "sp"), "tp"),
            P(("grp", "sp"), "tp"),
            P(("grp", "sp"), "tp"),
            P(("grp", "sp"), "tp"),
            P(("grp", "sp"), "tp"),
            P(("grp", "sp"), "tp"),
            P(None, "tp", ("grp", "sp")),
            P(None, "tp", ("grp", "sp")),
            P(("grp", "sp", "tp"), None),
            P(None, None, "tp"),
            P(),
            P("sp", "tp"),
            P("sp", "tp"),
            P("sp", "tp"),
        ),
        out_specs=P(("grp", "sp", "tp"), None),
        check_vma=False,
    )
```

```python
import functools

import jax
import jax.numpy as jnp
from jax import lax
from jax.experimental import pallas as pl
from jax.experimental.pallas import tpu as pltpu
from jax.sharding import PartitionSpec as P

DKA = 128
DKB = 64
DV = 256


EPS = 1e-06
NEG = -1e30


def summarize(key_heads, value_head_rows, input_log, forget_raw):
    cum_forget = jnp.cumsum(jax.nn.log_sigmoid(forget_raw), axis=1)
    offset_log = input_log - cum_forget
    block_sum = cum_forget[:, -1]
    block_max = block_sum + jnp.max(offset_log, axis=1)
    key_decay = jnp.exp(block_sum[:, None] + offset_log - block_max[:, None])
    scaled_keys = (key_heads.astype(jnp.float32) * jnp.transpose(key_decay)[:, :, None]).astype(
        jnp.bfloat16
    )
    block_memory_state = jnp.einsum(
        "eif,eiw->ifw", scaled_keys, value_head_rows, preferred_element_type=jnp.float32
    )
    return (block_memory_state, block_max, block_sum, offset_log)


def head_outputs(
    query_head_rows,
    key_heads,
    value_head_rows,
    outgate,
    offset_log,
    carried_over,
    mstate,
    key_width,
):
    length = query_head_rows.shape[0]
    run_max = jnp.maximum(lax.cummax(offset_log, axis=1), mstate[:, None])
    causal = jnp.arange(length)[:, None] >= jnp.arange(length)[None, :]
    exponent = jnp.where(causal[None], offset_log[:, None, :] - run_max[:, :, None], -jnp.inf)
    scores = jnp.einsum(
        "thk,shk->hts", query_head_rows, key_heads, preferred_element_type=jnp.float32
    )
    scores = scores * key_width ** (-0.5) * jnp.exp(exponent)
    weights_bf = scores.astype(jnp.bfloat16)
    inner_part = jnp.einsum(
        "hts,shv->thv", weights_bf, value_head_rows, preferred_element_type=jnp.float32
    )
    carried_portion = jnp.einsum(
        "pix,ixe->pie",
        query_head_rows,
        carried_over.astype(jnp.bfloat16),
        preferred_element_type=jnp.float32,
    ) * key_width ** (-0.5)
    carried_portion = (
        carried_portion * jnp.transpose(jnp.exp(mstate[:, None] - run_max))[:, :, None]
    )
    numerator = carried_portion + inner_part
    inv_rms = lax.rsqrt(jnp.mean(numerator * numerator, axis=2, keepdims=True) + EPS)
    gated_out = (
        numerator * inv_rms * jax.nn.sigmoid(outgate.astype(jnp.float32).reshape(numerator.shape))
    )
    return gated_out.reshape(length, -1).astype(jnp.bfloat16)


def shifted(value, axis, shift):
    count = lax.axis_size(axis)
    return lax.ppermute(value, axis, [(i, (i + shift) % count) for i in range(count)])


def swapped(value, axis):
    count = lax.axis_size(axis)
    return lax.ppermute(value, axis, [(i, i ^ 1) for i in range(count)])


def side_swapped(value):
    return swapped(value, "grp")


def column_shifted(value, shift):
    count = lax.axis_size("tp")
    return lax.ppermute(value, "tp", [(i, (i + 2 * shift) % count) for i in range(count)])


def split_wide(value):
    high = lax.reduce_precision(value, 8, 7)
    middle = lax.reduce_precision(value - high, 8, 7)
    return jnp.stack([high, middle, value - high - middle]).astype(jnp.bfloat16)


def entering(state_a, state_b, stats):
    count, mine = lax.axis_size("sp"), lax.axis_index("sp")
    heads, depth_a, width = state_a.shape
    depth_b = state_b.shape[1]
    terms = split_wide(stats).transpose(3, 0, 1, 2).reshape(heads, 1, 12)
    terms = jnp.pad(terms, ((0, 0), (0, 15), (0, width - 12)))
    packed = jnp.concatenate(
        [state_a.astype(jnp.bfloat16), state_b.astype(jnp.bfloat16), terms], axis=1
    )
    parts = [
        lax.ppermute(packed, "sp", [(i, i + step) for i in range(count - step)])
        for step in range(1, count)
    ]
    total = jnp.zeros_like(stats[1])
    highest = jnp.full_like(stats[0], NEG)
    logs = []
    for step in range(1, count):
        got = parts[step - 1][:, depth_a + depth_b, :12].astype(jnp.float32)
        stat = jnp.sum(got.reshape(heads, 3, 2, 2), axis=1).transpose(1, 2, 0)
        logs.append(jnp.where(step <= mine, stat[0] + total, NEG))
        total = total + stat[1]
        highest = jnp.maximum(highest, logs[-1])
    carried_a, carried_b = jnp.zeros_like(state_a), jnp.zeros_like(state_b)
    for step in range(1, count):
        weight = jnp.where(step <= mine, jnp.exp(logs[step - 1] - highest), 0.0)[:, :, None, None]
        part = parts[step - 1].astype(jnp.float32)
        carried_a += weight[0] * part[:, :depth_a]
        carried_b += weight[1] * part[:, depth_a : depth_a + depth_b]
    return carried_a, carried_b, highest


def scatter_pair(partial):
    chips = lax.axis_size("tp") // 2
    me = lax.axis_index("tp")
    chip, core = me // 2, me % 2
    parts = partial.reshape(2, chips, 2, -1, partial.shape[-1])
    away = lax.dynamic_index_in_dim(parts, 1 - core, 2, keepdims=False).astype(jnp.bfloat16)
    kept = lax.dynamic_index_in_dim(parts, core, 2, keepdims=False)
    got = swapped(away, "tp")
    totals = []
    for which in (1, 0):
        both = kept[which].astype(jnp.float32) + got[which].astype(jnp.float32)
        total = lax.dynamic_index_in_dim(both, chip, 0, keepdims=False)
        for step in range(1, chips):
            target = lax.rem(chip + step, chips)
            sent = lax.dynamic_index_in_dim(both, target, 0, keepdims=False).astype(jnp.bfloat16)
            total = total + column_shifted(sent, step).astype(jnp.float32)
        totals.append(total)
    return totals[1] + swapped(totals[0].astype(jnp.bfloat16), "sp").astype(jnp.float32)


def scatter_rows(partial):
    chips = lax.axis_size("tp") // 2
    me = lax.axis_index("tp")
    chip, core = me // 2, me % 2
    parts = partial.reshape(chips, 2, -1, partial.shape[-1])
    away = lax.dynamic_index_in_dim(parts, 1 - core, 1, keepdims=False).astype(jnp.bfloat16)
    kept = lax.dynamic_index_in_dim(parts, core, 1, keepdims=False)
    both = kept.astype(jnp.float32) + swapped(away, "tp").astype(jnp.float32)
    total = lax.dynamic_index_in_dim(both, chip, 0, keepdims=False)
    for step in range(1, chips):
        target = lax.rem(chip + step, chips)
        sent = lax.dynamic_index_in_dim(both, target, 0, keepdims=False).astype(jnp.bfloat16)
        total = total + column_shifted(sent, step).astype(jnp.float32)
    return total


def gather_rows(rows):
    chips = lax.axis_size("tp") // 2
    core = lax.axis_index("tp") % 2
    mine = jnp.stack([rows] + [column_shifted(rows, step) for step in range(1, chips)])
    other = swapped(mine, "tp")
    first = jnp.where(core == 0, mine, other)
    second = jnp.where(core == 0, other, mine)
    gathered = jnp.stack([first, second], axis=1)
    return gathered.reshape(-1, rows.shape[-1])


def by_owner(partial):
    chips = lax.axis_size("tp") // 2
    chip = lax.axis_index("tp") // 2
    parts = partial.reshape(chips, -1, partial.shape[-1])
    order = [
        lax.dynamic_index_in_dim(parts, lax.rem(chip - owner + chips, chips), 0)
        for owner in range(chips)
    ]
    return jnp.concatenate(order).reshape(partial.shape)


def local(
    query_a,
    key_a,
    query_b,
    key_b,
    values_a,
    values_b,
    outgate_a,
    outgate_b,
    input_pre,
    forget_pre,
    resid,
    out_proj,
    norm_gain,
    w_gate,
    w_up,
    w_down,
):
    tokens_dev = query_a.shape[0]
    heads_dev = query_a.shape[1] // DKA
    count, place, part = lax.axis_size("sp"), lax.axis_index("sp"), lax.axis_index("grp")
    depth, units = w_gate.shape
    half = units // 2
    side = lax.rem(place, 2)

    def columns(weight, step):
        target_side = lax.rem(place + step, 2)
        return lax.dynamic_slice_in_dim(weight, target_side * half, half, 1)

    lead = jnp.where(part == 0, w_gate, w_up)
    first_sent = columns(lead, 1)
    lead_parts = [None, shifted(first_sent, "sp", 1)]
    key_heads_a = key_a.reshape(tokens_dev, heads_dev, DKA)
    key_heads_b = key_b.reshape(tokens_dev, heads_dev, DKB)
    value_heads_a = values_a.reshape(tokens_dev, heads_dev, DV)
    value_heads_b = values_b.reshape(tokens_dev, heads_dev, DV)
    state_a, max_a, sum_a, offset_a = summarize(
        key_heads_a, value_heads_a, input_pre[0], forget_pre[0]
    )
    state_b, max_b, sum_b, offset_b = summarize(
        key_heads_b, value_heads_b, input_pre[1], forget_pre[1]
    )
    stats = jnp.stack([jnp.stack([max_a, max_b]), jnp.stack([sum_a, sum_b])])
    lead, w_down, state_a, state_b, stats = lax.optimization_barrier(
        (lead, w_down, state_a, state_b, stats)
    )
    carried_a, carried_b, mstate = entering(state_a, state_b, stats)
    for step in range(2, count):
        lead_parts.append(shifted(columns(lead, step), "sp", step))
    down_mine = lax.dynamic_slice_in_dim(w_down, part * (depth // 2), depth // 2, 0)
    down_parts = [None] + [
        shifted(columns(down_mine, step), "sp", step) for step in range(1, count)
    ]
    hidden_a = head_outputs(
        query_a.reshape(tokens_dev, heads_dev, DKA),
        key_heads_a,
        value_heads_a,
        outgate_a,
        offset_a,
        carried_a,
        mstate[0],
        DKA,
    )
    hidden_b = head_outputs(
        query_b.reshape(tokens_dev, heads_dev, DKB),
        key_heads_b,
        value_heads_b,
        outgate_b,
        offset_b,
        carried_b,
        mstate[1],
        DKB,
    )
    hidden = jnp.stack([hidden_a, hidden_b], axis=1).reshape(tokens_dev, -1)
    proj_weight = out_proj.reshape(out_proj.shape[0], -1)
    row_block = hidden
    attn_rows = scatter_rows(
        lax.dot_general(
            row_block, proj_weight, (((1,), (1,)), ((), ())), preferred_element_type=jnp.float32
        )
    )
    resid_sum = resid.astype(jnp.float32) + attn_rows
    normed = (
        resid_sum
        * lax.rsqrt(jnp.mean(resid_sum * resid_sum, axis=1, keepdims=True) + EPS)
        * norm_gain
    )
    normed = normed.astype(jnp.bfloat16)
    pair_normed = swapped(normed, "sp")
    own = lambda weight: lax.dynamic_slice_in_dim(weight, side * half, half, 1)
    own_trail = jnp.where(part == 0, own(w_up), own(w_gate))
    lead_parts[0] = own(lead)
    trail_parts = [own_trail] + [side_swapped(piece) for piece in lead_parts[1:]]
    other_down = lax.dynamic_slice_in_dim(w_down, (1 - part) * (depth // 2), depth // 2, 0)
    down_parts[0] = own(down_mine)
    down_other = [own(other_down)] + [side_swapped(piece) for piece in down_parts[1:]]

    def placed(pieces, offset, blocks):
        whole = jnp.zeros((blocks * depth, half), jnp.bfloat16)
        for step, (first, second) in enumerate(pieces):
            origin = lax.rem(place - step + count, count) * depth
            whole = lax.dynamic_update_slice_in_dim(whole, first, origin + part * offset, 0)
            if second is not None:
                whole = lax.dynamic_update_slice_in_dim(
                    whole, second, origin + (1 - part) * offset, 0
                )
        return whole

    lead_full = placed([(piece, None) for piece in lead_parts], 0, count)
    trail_full = placed([(piece, None) for piece in trail_parts], 0, count)
    down_full = placed(list(zip(down_parts, down_other)), depth // 2, count)
    rows = jnp.concatenate([gather_rows(normed), gather_rows(pair_normed)])
    lead_act = jnp.dot(rows, lead_full, preferred_element_type=jnp.float32)
    trail_act = jnp.dot(rows, trail_full, preferred_element_type=jnp.float32)
    gate_act = jnp.where(part == 0, lead_act, trail_act)
    up_act = jnp.where(part == 0, trail_act, lead_act)
    inner_act = (jax.nn.silu(gate_act) * up_act).astype(jnp.bfloat16)
    partial = lax.dot_general(
        inner_act, down_full, (((1,), (1,)), ((), ())), preferred_element_type=jnp.float32
    ).astype(jnp.bfloat16)
    partial = partial.reshape(2, -1, partial.shape[-1])
    partial = jnp.stack([by_owner(partial[0]), by_owner(partial[1])])
    return (resid_sum + scatter_pair(partial)).astype(jnp.bfloat16)


MESH = pl.DeviceIdType.MESH
NT = (((1,), (1,)), ((), ()))
TN = (((0,), (0,)), ((), ()))
F32 = jnp.float32
BF16 = jnp.bfloat16
SUBS = 2
LAG_B, LAG_C, LAG_D, RING = 2, 5, 8, 8
VMEM_BYTES = 60 * 2**20


SENDS = (
    (((0, 1),), ((1, 1), (2, 1), (3, 1)), ((0, 2), (1, 2), (0, 3), (1, 3)), ((2, 2), (3, 2), (2, 3), (3, 3)), ((4, 3), (4, 2), (4, 1), (5, 3), (5, 2), (5, 1))),
    (((0, 0), (1, 0), (2, 0), (3, 0), (0, 2), (1, 2)), ((2, 2), (3, 2)), ((0, 3), (1, 3), (2, 3), (3, 3), (4, 3), (4, 2), (5, 3), (5, 2)), ((4, 0), (5, 0)), ()),
    (((0, 0), (0, 1), (1, 0), (1, 1), (2, 0), (2, 1), (3, 0), (3, 1), (4, 0), (4, 1), (5, 0), (5, 1), (0, 3), (1, 3)), ((2, 3), (3, 3)), (), ((4, 3), (5, 3)), ()),
    (((0, 0), (0, 1), (0, 2), (1, 0), (1, 1), (1, 2), (2, 0), (2, 1), (2, 2), (3, 0), (3, 1), (3, 2)), (), (), (), ((4, 0), (4, 1), (4, 2), (5, 0), (5, 1), (5, 2))),
)
FORWARDS = (
    ((), ((0, 3),), ((0, 1), (0, 2), (1, 3), (1, 1)), ((2, 1), (2, 3), (3, 1), (1, 2)), ((3, 3), (2, 2)), (), ((3, 2), (4, 1)), (), ()),
    (((0, 0), (0, 3)), (), ((1, 0), (2, 0), (1, 3), (3, 0), (0, 2)), ((2, 3),), ((3, 3),), ((1, 2),), ((2, 2),), (), ((3, 2),)),
    (((0, 1), (1, 1), (0, 3)), (), ((2, 1), (1, 3), (0, 0), (1, 0)), ((2, 3), (3, 1), (3, 3)), ((2, 0), (3, 0)), (), (), (), ()),
    (((0, 2), (1, 2)), (), ((2, 2), (0, 0), (1, 0), (3, 2)), ((0, 1),), ((2, 0), (3, 0), (1, 1), (2, 1)), ((3, 1),), ((4, 0),), (), ()),
)
ROUNDS = (
    ((1, 0), (3, 0), (1, 1), (0, 0), (2, 0), (3, 1), (2, 1), (0, 1)),
    ((3, 0), (0, 0), (2, 0), (0, 1), (3, 1), (2, 1), (1, 0), (1, 1)),
)


def scan_lanes(value, combine, neutral):
    length = value.shape[1]
    lane = lax.broadcasted_iota(jnp.int32, value.shape, 1)
    step = 1
    while step < length:
        moved = jnp.where(lane >= step, pltpu.roll(value, step, 1), neutral)
        value = combine(value, moved)
        step *= 2
    return value


def fused_body(
    sizes,
    query_a,
    key_a,
    query_b,
    key_b,
    values_a,
    values_b,
    outgate_a,
    outgate_b,
    input_pre,
    forget_pre,
    resid,
    out_proj,
    gain,
    w_gate,
    w_up,
    w_down,
    out_ref,
    qa, ka, qb, kb, va, vb, oga, ogb, inp, fgt, res, proj, gn,
    wg, wu, wd,
    cols, offs, bstate, st_out, st_in, stat_out, stat_in, intra, hidden,
    part1, keep1, dsend1, drecv1, xsend1, xrecv1, rsum,
    rows, act, inner, part2, keep2, dsend2, drecv2, xsend2, xrecv2, zsend2, zrecv2,
    lsem, zs, zr, ys, yr, cs, cr, d1s, d1r, x1s, x1r, ags, agr,
    d2s, d2r, x2s, x2r, z2s, z2r,
):
    count, tokens, heads, depth, half, block, chunk1, _ = sizes
    g, s, t = lax.axis_index("grp"), lax.axis_index("sp"), lax.axis_index("tp")
    x, c = lax.div(t, 2), lax.rem(t, 2)
    core_peer = (g, s, t + 1 - 2 * c)
    x_peer = (g, s, t + 2 - 4 * x)
    y_peer = (1 - g, s, t)
    pair = (g, s + 1 - 2 * lax.rem(s, 2), t)
    part_rows = depth // 2
    sub_rows = part_rows // SUBS

    def remote(src, dst, send, recv, device):
        return pltpu.make_async_remote_copy(
            src_ref=src, dst_ref=dst, send_sem=send, recv_sem=recv,
            device_id=device, device_id_type=MESH,
        )

    barrier = pltpu.get_barrier_semaphore()
    for device in (core_peer, x_peer, y_peer):
        pl.semaphore_signal(barrier, inc=1, device_id=device, device_id_type=MESH)
    for place in range(count):
        @pl.when(place != s)
        def _():
            pl.semaphore_signal(barrier, inc=1, device_id=(g, place, t), device_id_type=MESH)

    side = lax.rem(s, 2)
    own_cols = pl.ds(pl.multiple_of(side * half, 128), half)
    own_rows = pl.ds(pl.multiple_of(s * depth, depth), depth)
    loads = [
        (input_pre, inp), (forget_pre, fgt), (key_a, ka), (key_b, kb), (values_a, va),
        (values_b, vb), (query_a, qa), (query_b, qb), (outgate_a, oga), (outgate_b, ogb),
        (out_proj, proj), (resid, res), (gain, gn),
        (w_gate.at[:, own_cols], wg.at[own_rows]),
        (w_up.at[:, own_cols], wu.at[own_rows]),
        (w_down.at[:, own_cols], wd.at[own_rows]),
    ]
    local = [pltpu.make_async_copy(a, b, lsem.at[i]) for i, (a, b) in enumerate(loads)]
    for copy in local[:8]:
        copy.start()

    whole_of = (wg,) * SUBS + (wu,) * SUBS + (wd,) * SUBS
    held_of = (w_gate,) * SUBS + (w_up,) * SUBS + (w_down,) * SUBS
    gates, ups, _ = (range(i * SUBS, (i + 1) * SUBS) for i in range(3))

    def piece_rows(pid, source, which):
        start = source * depth + which * part_rows + (pid % SUBS) * sub_rows
        return pl.ds(pl.multiple_of(start, sub_rows), sub_rows)

    def z_copy(pid, dest):
        start = g * part_rows + (pid % SUBS) * sub_rows
        src = held_of[pid].at[
            pl.ds(pl.multiple_of(start, sub_rows), sub_rows), pl.ds((dest % 2) * half, half)
        ]
        return remote(
            src, whole_of[pid].at[piece_rows(pid, s, g)],
            zs.at[pid, dest], zr.at[pid, s], (g, dest, t),
        )

    def y_copy(pid, source, which):
        place = whole_of[pid].at[piece_rows(pid, source, which)]
        return remote(place, place, ys.at[pid, source], yr.at[pid, source], y_peer)

    def arrived_z(pid, source):
        place = whole_of[pid].at[piece_rows(pid, source, g)]
        remote(place, place, zs.at[pid, source], zr.at[pid, source], y_peer).wait_recv()

    last = count - 1

    def issue(point):
        for place, plan in enumerate(SENDS):
            @pl.when(s == place)
            def _():
                for pid, dest in plan[point]:
                    z_copy(pid, dest).start()

    def serve(point):
        for place, plan in enumerate(FORWARDS):
            @pl.when(s == place)
            def _():
                for pid, source in plan[point]:
                    arrived_z(pid, source)
                    y_copy(pid, source, g).start()

    pl.semaphore_wait(barrier, 3 + count - 1)
    issue(0)

    for i in range(2):
        local[i].wait()
    quad = lambda ref: jnp.concatenate([ref[0], ref[1], ref[0], ref[1]], axis=0)
    raw_forget, raw_input = quad(fgt), quad(inp)
    log_forget = jnp.minimum(raw_forget, 0.0) - jnp.log1p(jnp.exp(-jnp.abs(raw_forget)))
    cum = scan_lanes(log_forget, lambda a, b: a + b, 0.0)
    offset = raw_input - cum
    run = scan_lanes(offset, jnp.maximum, NEG)
    fsum = cum[:, tokens - 1 : tokens]
    top = run[:, tokens - 1 : tokens]
    bmax = fsum + top
    decay = jnp.exp(offset - top)
    offs[...] = offset
    group = 2 * heads
    cols[...] = jnp.transpose(jnp.concatenate([decay[:group], run[:group]], axis=0))

    for i in range(2, 6):
        local[i].wait()
    head_lane = lax.div(lax.broadcasted_iota(jnp.int32, (tokens, heads * DKB), 1), DKB)
    state_of = []
    for h in range(heads):
        column = cols[:, h : h + 1]
        scaled = (ka[:, h * DKA : (h + 1) * DKA].astype(F32) * column).astype(BF16)
        state = lax.dot_general(
            scaled, va[:, h * DV : (h + 1) * DV], TN, preferred_element_type=F32
        )
        bstate[h * DKA : (h + 1) * DKA, :] = state
        state_of.append((h * DKA, DKA, h))
    base_b = heads * DKA
    for h in range(heads):
        column = cols[:, heads + h : heads + h + 1]
        scaled = (kb[...].astype(F32) * column).astype(BF16)
        state = lax.dot_general(
            scaled, vb[:, h * DV : (h + 1) * DV], TN, preferred_element_type=F32
        )
        bstate[base_b + h * DKB : base_b + (h + 1) * DKB, :] = state[h * DKB : (h + 1) * DKB]
        state_of.append((base_b + h * DKB, DKB, heads + h))

    after_peer = (g, jnp.minimum(s + 1, last), t)
    chain = [
        remote(
            st_out.at[pl.ds(start, size)], st_in.at[pl.ds(start, size)],
            cs.at[h], cr.at[h], after_peer,
        )
        for start, size, h in state_of
    ]
    chain_stat = remote(stat_out, stat_in, cs.at[group], cr.at[group], after_peer)
    wide = lambda row: jnp.concatenate([row] * (DV // 128), axis=1)

    def combine_stat():
        before = stat_in[...]
        total = before + fsum
        after = jnp.maximum(total, bmax)
        stat_out[...] = after
        chain_stat.start()
        return jnp.exp(total - after), jnp.exp(jnp.broadcast_to(bmax, total.shape) - after)

    def combine_head(i, keep_old, keep_new):
        start, size, h = state_of[i]
        st_out[start : start + size, :] = (
            wide(keep_old[h : h + 1, :]) * st_in[start : start + size, :].astype(F32)
            + wide(keep_new[h : h + 1, :]) * bstate[start : start + size, :]
        ).astype(BF16)
        chain[i].start()

    @pl.when(s == 0)
    def _():
        st_in[...] = jnp.zeros_like(st_in)
        stat_in[...] = jnp.full_like(stat_in, NEG)
        keeps = combine_stat()
        for i in range(group):
            combine_head(i, *keeps)
        issue(1)

    for copy in local[8:]:
        copy.start()
    for i in range(6, 8):
        local[i].wait()
    causal = lax.broadcasted_iota(jnp.int32, (tokens, tokens), 0) >= lax.broadcasted_iota(
        jnp.int32, (tokens, tokens), 1
    )

    def query_of(h):
        if h < heads:
            return qa[:, h * DKA : (h + 1) * DKA]
        return jnp.where(head_lane == h - heads, qb[...], jnp.zeros_like(qb[...]))

    for h in range(group):
        key = ka[:, h * DKA : (h + 1) * DKA] if h < heads else kb[...]
        value_ref, at = (va, h) if h < heads else (vb, h - heads)
        width = DKA if h < heads else DKB
        scores = lax.dot_general(query_of(h), key, NT, preferred_element_type=F32)
        exponent = jnp.where(causal, offs[h : h + 1, :] - cols[:, group + h : group + h + 1], NEG)
        weights = (scores * width ** (-0.5) * jnp.exp(exponent)).astype(BF16)
        intra[h] = jnp.dot(
            weights, value_ref[:, at * DV : (at + 1) * DV], preferred_element_type=F32
        )

    @pl.when(jnp.logical_and(s > 0, s < last))
    def _():
        chain_stat.wait_recv()
        keeps = combine_stat()
        for i in range(group):
            chain[i].wait_recv()
            combine_head(i, *keeps)
        issue(1)

    @pl.when(s == last)
    def _():
        chain_stat.wait_recv()
        for copy in chain:
            copy.wait_recv()

    serve(0)
    for i in range(8, 10):
        local[i].wait()
    for h in range(group):
        width = DKA if h < heads else DKB
        gate_ref, at = (oga, h) if h < heads else (ogb, h - heads)
        state = (
            st_in[h * DKA : (h + 1) * DKA, :] if h < heads else st_in[base_b:, :]
        )
        entering_max = stat_in[h : h + 1, 0:1]
        own_max = cols[:, group + h : group + h + 1]
        top_max = jnp.maximum(own_max, entering_max)
        carried = jnp.dot(query_of(h), state, preferred_element_type=F32)
        numer = carried * (width ** (-0.5) * jnp.exp(entering_max - top_max)) + intra[
            h
        ] * jnp.exp(own_max - top_max)
        inv = lax.rsqrt(jnp.mean(numer * numer, axis=1, keepdims=True) + EPS)
        gated = numer * inv * jax.nn.sigmoid(gate_ref[:, at * DV : (at + 1) * DV].astype(F32))
        hidden[:, h * DV : (h + 1) * DV] = gated.astype(BF16)

    serve(1)

    for i in range(10, 13):
        local[i].wait()
    chunks1 = proj.shape[0] // chunk1

    def block_rows(chip, core):
        return pl.ds(pl.multiple_of((2 * chip + core) * block, 8), block)

    def d1(j):
        return remote(dsend1.at[j], drecv1.at[j], d1s.at[j], d1r.at[j], core_peer)

    def x1(j):
        return remote(xsend1.at[j], xrecv1.at[j], x1s.at[j], x1r.at[j], x_peer)

    def attn_step(j, carry):
        @pl.when(j < chunks1)
        def _():
            weight = proj[pl.ds(pl.multiple_of(j * chunk1, chunk1), chunk1)]
            part1[...] = lax.dot_general(
                hidden[...], weight.reshape(chunk1, hidden.shape[1]), NT,
                preferred_element_type=F32,
            )
            for role in range(2):
                chip = x if role == 0 else 1 - x
                dsend1[j, role] = part1[block_rows(chip, 1 - c)].astype(BF16)
                keep1[j, role] = part1[block_rows(chip, c)]
            d1(j).start()

        @pl.when(j >= 1)
        def _():
            k = j - 1
            d1(k).wait_recv()
            xsend1[k] = (keep1[k, 1] + drecv1[k, 1].astype(F32)).astype(BF16)
            x1(k).start()
            keep1[k, 0] = keep1[k, 0] + drecv1[k, 0].astype(F32)

        return carry

    lax.fori_loop(0, chunks1 + 1, attn_step, 0)
    issue(2)
    serve(2)
    for j in range(chunks1):
        span = slice(j * chunk1, (j + 1) * chunk1)
        x1(j).wait_recv()
        rsum[:, span] = res[:, span].astype(F32) + keep1[j, 0] + xrecv1[j].astype(F32)
    summed = rsum[...]
    scale = lax.rsqrt(jnp.mean(summed * summed, axis=1, keepdims=True) + EPS)
    mine = block_rows(x, c)
    rows[0, mine] = (summed * scale * gn[...]).astype(BF16)

    def move(kind, src_place, dst_place, chip, core, device):
        return remote(
            rows.at[src_place, block_rows(chip, core)],
            rows.at[dst_place, block_rows(chip, core)],
            ags.at[kind], agr.at[kind], device,
        )

    own_z = move(2, 0, 1, x, c, pair)
    own_x = move(1, 0, 0, x, c, x_peer)
    own_d = move(0, 0, 0, x, c, core_peer)
    own_z.start()
    own_x.start()
    own_d.start()
    issue(3)

    def arrived(kind, place, chip, core):
        move(kind, place, place, chip, core, core_peer).wait_recv()

    serve(3)
    arrived(1, 0, 1 - x, c)
    fwd_x = move(3, 0, 0, 1 - x, c, core_peer)
    fwd_x.start()
    serve(4)
    arrived(2, 1, x, c)
    fwd_zx = move(5, 1, 1, x, c, x_peer)
    fwd_zd = move(4, 1, 1, x, c, core_peer)
    fwd_zx.start()
    fwd_zd.start()
    serve(5)

    def take_y(pids):
        for place in range(count):
            @pl.when(place != s)
            def _():
                for pid in pids:
                    y_copy(pid, place, 1 - g).wait_recv()

    for i in range(13, 16):
        local[i].wait()
    take_y(gates)
    arrived(0, 0, x, 1 - c)
    arrived(3, 0, 1 - x, 1 - c)
    act[0] = jnp.dot(rows[0], wg[...], preferred_element_type=F32)
    serve(6)
    arrived(5, 1, 1 - x, c)
    issue(4)
    fwd_xd = move(6, 1, 1, 1 - x, c, core_peer)
    fwd_xd.start()
    serve(7)
    arrived(4, 1, x, 1 - c)
    arrived(6, 1, 1 - x, 1 - c)
    act[1] = jnp.dot(rows[1], wg[...], preferred_element_type=F32)
    serve(8)
    take_y(ups)

    def up_step(p, carry):
        gate = act[p]
        up = jnp.dot(rows[p], wu[...], preferred_element_type=F32)
        start = pl.multiple_of(p * tokens, tokens)
        inner[pl.ds(start, tokens), :] = (gate / (1.0 + jnp.exp(-gate)) * up).astype(BF16)
        return carry

    lax.fori_loop(0, 2, up_step, 0)

    rounds = count * SUBS
    chunks2 = 2 * rounds

    def look(table, k):
        value = jnp.int32(table[0])
        for i, entry in enumerate(table[1:], 1):
            value = jnp.where(k == i, entry, value)
        return value

    low = s < count // 2

    def place_of(p):
        is_y = jnp.logical_or(
            jnp.logical_and(p > 0, lax.rem(p, 2) == 0), p == chunks2 - 1
        )
        r = jnp.where(
            p == chunks2 - 1, rounds - 1,
            jnp.where(is_y, lax.div(p, 2) - 1, lax.div(p + 1, 2)),
        )
        r = jnp.maximum(r, 0)
        b, sub = (
            jnp.where(low, *(look([pick[i] for pick in order], r) for order in ROUNDS))
            for i in range(2)
        )
        which = jnp.where(is_y, 1 - g, g)
        return b, sub, which, is_y, r

    def is_late(r):
        value = jnp.bool_(False)
        for place, plan in enumerate(FORWARDS):
            done = {pair_ for point in plan for pair_ in point}
            for k, (b, sub) in enumerate(ROUNDS[0 if place < count // 2 else 1]):
                if b != place and (2 * SUBS + sub, b) not in done:
                    value = jnp.logical_or(value, jnp.logical_and(s == place, r == k))
        return value

    def down_rows(p):
        b, sub, which, _, _ = place_of(p)
        return b * depth + which * part_rows + sub * sub_rows

    def d2(k):
        return remote(dsend2.at[k], drecv2.at[k], d2s.at[k], d2r.at[k], core_peer)

    def x2(k):
        return remote(xsend2.at[k], xrecv2.at[k], x2s.at[k], x2r.at[k], x_peer)

    def z2(k):
        return remote(zsend2.at[k], zrecv2.at[k], z2s.at[k], z2r.at[k], pair)

    def down_step(p, carry):
        @pl.when(p < chunks2)
        def _():
            b, sub, _, is_y, r = place_of(p)
            start = pl.multiple_of(down_rows(p), sub_rows)
            spot = wd.at[pl.ds(start, sub_rows)]
            pid = 2 * SUBS + sub
            z_in = remote(spot, spot, zs.at[pid, b], zr.at[pid, b], y_peer)
            y_both = remote(spot, spot, ys.at[pid, b], yr.at[pid, b], y_peer)

            @pl.when(jnp.logical_and(b != s, jnp.logical_not(is_y)))
            def _():
                @pl.when(is_late(r))
                def _():
                    z_in.wait_recv()
                    y_both.start()

            @pl.when(jnp.logical_and(b != s, is_y))
            def _():
                y_both.wait_recv()

            part2[...] = lax.dot_general(
                inner[...], wd[pl.ds(start, sub_rows), :], NT, preferred_element_type=F32
            )
            ring = lax.rem(p, RING)
            for place in range(2):
                for role in range(2):
                    chip = x if role == 0 else 1 - x
                    send = pl.multiple_of(place * tokens + (2 * chip + 1 - c) * block, 8)
                    hold = pl.multiple_of(place * tokens + (2 * chip + c) * block, 8)
                    dsend2[p, 2 * place + role] = part2[pl.ds(send, block)].astype(BF16)
                    keep2[ring, 2 * place + role] = part2[pl.ds(hold, block)]
            d2(p).start()

        @pl.when(jnp.logical_and(p >= LAG_B, p < chunks2 + LAG_B))
        def _():
            k = p - LAG_B
            ring = lax.rem(k, RING)
            d2(k).wait_recv()
            for place in range(2):
                xsend2[k, place] = (
                    keep2[ring, 2 * place + 1] + drecv2[k, 2 * place + 1].astype(F32)
                ).astype(BF16)
            x2(k).start()
            for place in range(2):
                keep2[ring, 2 * place] = keep2[ring, 2 * place] + drecv2[
                    k, 2 * place
                ].astype(F32)

        @pl.when(jnp.logical_and(p >= LAG_C, p < chunks2 + LAG_C))
        def _():
            k = p - LAG_C
            ring = lax.rem(k, RING)
            x2(k).wait_recv()
            zsend2[k] = (keep2[ring, 2] + xrecv2[k, 1].astype(F32)).astype(BF16)
            z2(k).start()
            span = pl.ds(pl.multiple_of(down_rows(k), sub_rows), sub_rows)
            rsum[:, span] = rsum[:, span] + keep2[ring, 0] + xrecv2[k, 0].astype(F32)

        @pl.when(p >= LAG_D)
        def _():
            k = p - LAG_D
            z2(k).wait_recv()
            span = pl.ds(pl.multiple_of(down_rows(k), sub_rows), sub_rows)
            out_ref[:, span] = (rsum[:, span] + zrecv2[k].astype(F32)).astype(BF16)

        return carry

    lax.fori_loop(0, chunks2 + LAG_D, down_step, 0)

    for pid in range(3 * SUBS):
        for dest in range(count):
            @pl.when(dest != s)
            def _():
                z_copy(pid, dest).wait_send()
                y_copy(pid, dest, g).wait_send()

    @pl.when(s < last)
    def _():
        chain_stat.wait_send()
        for copy in chain:
            copy.wait_send()

    for copy in (own_z, own_x, own_d, fwd_x, fwd_zx, fwd_zd, fwd_xd):
        copy.wait_send()
    for j in range(chunks1):
        d1(j).wait_send()
        x1(j).wait_send()

    def drain(k, carry):
        d2(k).wait_send()
        x2(k).wait_send()
        z2(k).wait_send()
        return carry

    lax.fori_loop(0, chunks2, drain, 0)


def fused(*args):
    query_a, _, _, _, _ = args[:5]
    resid, w_gate = args[10], args[13]
    count = lax.axis_size("sp")
    tokens = query_a.shape[0]
    heads = query_a.shape[1] // DKA
    depth, units = w_gate.shape
    half = units // 2
    block, width = resid.shape
    chunk1 = width // 4
    chunk2 = depth // 2 // SUBS
    chunks1, chunks2 = width // chunk1, width // chunk2
    group = 2 * heads
    state_rows = heads * (DKA + DKB)
    sizes = (count, tokens, heads, depth, half, block, chunk1, chunk2)
    args = list(args)
    args[12] = args[12].reshape(1, width)
    vmem = lambda *shape, kind=BF16: pltpu.VMEM(shape, kind)
    dma = pltpu.SemaphoreType.DMA
    pieces = (3 * SUBS, count)
    copies = [args[i] for i in (0, 1, 2, 3, 4, 5, 6, 7, 8, 9, 10, 11, 12)]
    scratch = [pltpu.VMEM(a.shape, a.dtype) for a in copies]
    scratch += [vmem(width, half), vmem(width, half), vmem(width, half)]
    scratch += [
        vmem(tokens, 2 * group, kind=F32),
        vmem(2 * group, tokens, kind=F32),
        vmem(state_rows, DV, kind=F32),
        vmem(state_rows, DV),
        vmem(state_rows, DV),
        vmem(2 * group, 128, kind=F32),
        vmem(2 * group, 128, kind=F32),
        vmem(group, tokens, DV, kind=F32),
        vmem(tokens, group * DV),
        vmem(tokens, chunk1, kind=F32),
        vmem(chunks1, 2, block, chunk1, kind=F32),
        vmem(chunks1, 2, block, chunk1),
        vmem(chunks1, 2, block, chunk1),
        vmem(chunks1, block, chunk1),
        vmem(chunks1, block, chunk1),
        vmem(block, width, kind=F32),
        vmem(2, tokens, width),
        vmem(2, tokens, half, kind=F32),
        vmem(2 * tokens, half),
        vmem(2 * tokens, chunk2, kind=F32),
        vmem(RING, 4, block, chunk2, kind=F32),
        vmem(chunks2, 4, block, chunk2),
        vmem(chunks2, 4, block, chunk2),
        vmem(chunks2, 2, block, chunk2),
        vmem(chunks2, 2, block, chunk2),
        vmem(chunks2, block, chunk2),
        vmem(chunks2, block, chunk2),
    ]
    scratch += [dma((16,)), dma(pieces), dma(pieces), dma(pieces), dma(pieces), dma((group + 1,)), dma((group + 1,))]
    scratch += [dma((chunks1,))] * 4 + [dma((7,))] * 2 + [dma((chunks2,))] * 6
    return pl.pallas_call(
        functools.partial(fused_body, sizes),
        out_shape=jax.ShapeDtypeStruct(resid.shape, BF16),
        in_specs=[pl.BlockSpec(memory_space=pl.ANY)] * len(args),
        out_specs=pl.BlockSpec(memory_space=pltpu.VMEM),
        scratch_shapes=scratch,
        compiler_params=pltpu.CompilerParams(
            collective_id=0, has_side_effects=True, vmem_limit_bytes=VMEM_BYTES
        ),
    )(*args)


def layer(*args):
    return local(*args)


def solution(mesh):
    few = mesh.shape["sp"] == 4 and mesh.shape["tp"] == 4
    return jax.shard_map(
        fused if few else layer,
        mesh=mesh,
        in_specs=(
            P(("grp", "sp"), "tp"),
            P(("grp", "sp"), "tp"),
            P(("grp", "sp"), "tp"),
            P(("grp", "sp"), "tp"),
            P(("grp", "sp"), "tp"),
            P(("grp", "sp"), "tp"),
            P(("grp", "sp"), "tp"),
            P(("grp", "sp"), "tp"),
            P(None, "tp", ("grp", "sp")),
            P(None, "tp", ("grp", "sp")),
            P(("grp", "sp", "tp"), None),
            P(None, None, "tp"),
            P(),
            P("sp", "tp"),
            P("sp", "tp"),
            P("sp", "tp"),
        ),
        out_specs=P(("grp", "sp", "tp"), None),
        check_vma=False,
    )
```

```python
import functools

import jax
import jax.numpy as jnp
from jax import lax
from jax.experimental import pallas as pl
from jax.experimental.pallas import tpu as pltpu
from jax.sharding import PartitionSpec as P

DKA = 128
DKB = 64
DV = 256


EPS = 1e-06
NEG = -1e30


def summarize(key_heads, value_head_rows, input_log, forget_raw):
    cum_forget = jnp.cumsum(jax.nn.log_sigmoid(forget_raw), axis=1)
    offset_log = input_log - cum_forget
    block_sum = cum_forget[:, -1]
    block_max = block_sum + jnp.max(offset_log, axis=1)
    key_decay = jnp.exp(block_sum[:, None] + offset_log - block_max[:, None])
    scaled_keys = (key_heads.astype(jnp.float32) * jnp.transpose(key_decay)[:, :, None]).astype(
        jnp.bfloat16
    )
    block_memory_state = jnp.einsum(
        "eif,eiw->ifw", scaled_keys, value_head_rows, preferred_element_type=jnp.float32
    )
    return (block_memory_state, block_max, block_sum, offset_log)


def head_outputs(
    query_head_rows,
    key_heads,
    value_head_rows,
    outgate,
    offset_log,
    carried_over,
    mstate,
    key_width,
):
    length = query_head_rows.shape[0]
    run_max = jnp.maximum(lax.cummax(offset_log, axis=1), mstate[:, None])
    causal = jnp.arange(length)[:, None] >= jnp.arange(length)[None, :]
    exponent = jnp.where(causal[None], offset_log[:, None, :] - run_max[:, :, None], -jnp.inf)
    scores = jnp.einsum(
        "thk,shk->hts", query_head_rows, key_heads, preferred_element_type=jnp.float32
    )
    scores = scores * key_width ** (-0.5) * jnp.exp(exponent)
    weights_bf = scores.astype(jnp.bfloat16)
    inner_part = jnp.einsum(
        "hts,shv->thv", weights_bf, value_head_rows, preferred_element_type=jnp.float32
    )
    carried_portion = jnp.einsum(
        "pix,ixe->pie",
        query_head_rows,
        carried_over.astype(jnp.bfloat16),
        preferred_element_type=jnp.float32,
    ) * key_width ** (-0.5)
    carried_portion = (
        carried_portion * jnp.transpose(jnp.exp(mstate[:, None] - run_max))[:, :, None]
    )
    numerator = carried_portion + inner_part
    inv_rms = lax.rsqrt(jnp.mean(numerator * numerator, axis=2, keepdims=True) + EPS)
    gated_out = (
        numerator * inv_rms * jax.nn.sigmoid(outgate.astype(jnp.float32).reshape(numerator.shape))
    )
    return gated_out.reshape(length, -1).astype(jnp.bfloat16)


def shifted(value, axis, shift):
    count = lax.axis_size(axis)
    return lax.ppermute(value, axis, [(i, (i + shift) % count) for i in range(count)])


def swapped(value, axis):
    count = lax.axis_size(axis)
    return lax.ppermute(value, axis, [(i, i ^ 1) for i in range(count)])


def side_swapped(value):
    return swapped(value, "grp")


def column_shifted(value, shift):
    count = lax.axis_size("tp")
    return lax.ppermute(value, "tp", [(i, (i + 2 * shift) % count) for i in range(count)])


def split_wide(value):
    high = lax.reduce_precision(value, 8, 7)
    middle = lax.reduce_precision(value - high, 8, 7)
    return jnp.stack([high, middle, value - high - middle]).astype(jnp.bfloat16)


def entering(state_a, state_b, stats):
    count, mine = lax.axis_size("sp"), lax.axis_index("sp")
    heads, depth_a, width = state_a.shape
    depth_b = state_b.shape[1]
    terms = split_wide(stats).transpose(3, 0, 1, 2).reshape(heads, 1, 12)
    terms = jnp.pad(terms, ((0, 0), (0, 15), (0, width - 12)))
    packed = jnp.concatenate(
        [state_a.astype(jnp.bfloat16), state_b.astype(jnp.bfloat16), terms], axis=1
    )
    parts = [
        lax.ppermute(packed, "sp", [(i, i + step) for i in range(count - step)])
        for step in range(1, count)
    ]
    total = jnp.zeros_like(stats[1])
    highest = jnp.full_like(stats[0], NEG)
    logs = []
    for step in range(1, count):
        got = parts[step - 1][:, depth_a + depth_b, :12].astype(jnp.float32)
        stat = jnp.sum(got.reshape(heads, 3, 2, 2), axis=1).transpose(1, 2, 0)
        logs.append(jnp.where(step <= mine, stat[0] + total, NEG))
        total = total + stat[1]
        highest = jnp.maximum(highest, logs[-1])
    carried_a, carried_b = jnp.zeros_like(state_a), jnp.zeros_like(state_b)
    for step in range(1, count):
        weight = jnp.where(step <= mine, jnp.exp(logs[step - 1] - highest), 0.0)[:, :, None, None]
        part = parts[step - 1].astype(jnp.float32)
        carried_a += weight[0] * part[:, :depth_a]
        carried_b += weight[1] * part[:, depth_a : depth_a + depth_b]
    return carried_a, carried_b, highest


def scatter_pair(partial):
    chips = lax.axis_size("tp") // 2
    me = lax.axis_index("tp")
    chip, core = me // 2, me % 2
    parts = partial.reshape(2, chips, 2, -1, partial.shape[-1])
    away = lax.dynamic_index_in_dim(parts, 1 - core, 2, keepdims=False).astype(jnp.bfloat16)
    kept = lax.dynamic_index_in_dim(parts, core, 2, keepdims=False)
    got = swapped(away, "tp")
    totals = []
    for which in (1, 0):
        both = kept[which].astype(jnp.float32) + got[which].astype(jnp.float32)
        total = lax.dynamic_index_in_dim(both, chip, 0, keepdims=False)
        for step in range(1, chips):
            target = lax.rem(chip + step, chips)
            sent = lax.dynamic_index_in_dim(both, target, 0, keepdims=False).astype(jnp.bfloat16)
            total = total + column_shifted(sent, step).astype(jnp.float32)
        totals.append(total)
    return totals[1] + swapped(totals[0].astype(jnp.bfloat16), "sp").astype(jnp.float32)


def scatter_rows(partial):
    chips = lax.axis_size("tp") // 2
    me = lax.axis_index("tp")
    chip, core = me // 2, me % 2
    parts = partial.reshape(chips, 2, -1, partial.shape[-1])
    away = lax.dynamic_index_in_dim(parts, 1 - core, 1, keepdims=False).astype(jnp.bfloat16)
    kept = lax.dynamic_index_in_dim(parts, core, 1, keepdims=False)
    both = kept.astype(jnp.float32) + swapped(away, "tp").astype(jnp.float32)
    total = lax.dynamic_index_in_dim(both, chip, 0, keepdims=False)
    for step in range(1, chips):
        target = lax.rem(chip + step, chips)
        sent = lax.dynamic_index_in_dim(both, target, 0, keepdims=False).astype(jnp.bfloat16)
        total = total + column_shifted(sent, step).astype(jnp.float32)
    return total


def gather_rows(rows):
    chips = lax.axis_size("tp") // 2
    core = lax.axis_index("tp") % 2
    mine = jnp.stack([rows] + [column_shifted(rows, step) for step in range(1, chips)])
    other = swapped(mine, "tp")
    first = jnp.where(core == 0, mine, other)
    second = jnp.where(core == 0, other, mine)
    gathered = jnp.stack([first, second], axis=1)
    return gathered.reshape(-1, rows.shape[-1])


def by_owner(partial):
    chips = lax.axis_size("tp") // 2
    chip = lax.axis_index("tp") // 2
    parts = partial.reshape(chips, -1, partial.shape[-1])
    order = [
        lax.dynamic_index_in_dim(parts, lax.rem(chip - owner + chips, chips), 0)
        for owner in range(chips)
    ]
    return jnp.concatenate(order).reshape(partial.shape)


def local(
    query_a,
    key_a,
    query_b,
    key_b,
    values_a,
    values_b,
    outgate_a,
    outgate_b,
    input_pre,
    forget_pre,
    resid,
    out_proj,
    norm_gain,
    w_gate,
    w_up,
    w_down,
):
    tokens_dev = query_a.shape[0]
    heads_dev = query_a.shape[1] // DKA
    count, place, part = lax.axis_size("sp"), lax.axis_index("sp"), lax.axis_index("grp")
    depth, units = w_gate.shape
    half = units // 2
    side = lax.rem(place, 2)

    def columns(weight, step):
        target_side = lax.rem(place + step, 2)
        return lax.dynamic_slice_in_dim(weight, target_side * half, half, 1)

    lead = jnp.where(part == 0, w_gate, w_up)
    first_sent = columns(lead, 1)
    lead_parts = [None, shifted(first_sent, "sp", 1)]
    key_heads_a = key_a.reshape(tokens_dev, heads_dev, DKA)
    key_heads_b = key_b.reshape(tokens_dev, heads_dev, DKB)
    value_heads_a = values_a.reshape(tokens_dev, heads_dev, DV)
    value_heads_b = values_b.reshape(tokens_dev, heads_dev, DV)
    state_a, max_a, sum_a, offset_a = summarize(
        key_heads_a, value_heads_a, input_pre[0], forget_pre[0]
    )
    state_b, max_b, sum_b, offset_b = summarize(
        key_heads_b, value_heads_b, input_pre[1], forget_pre[1]
    )
    stats = jnp.stack([jnp.stack([max_a, max_b]), jnp.stack([sum_a, sum_b])])
    lead, w_down, state_a, state_b, stats = lax.optimization_barrier(
        (lead, w_down, state_a, state_b, stats)
    )
    carried_a, carried_b, mstate = entering(state_a, state_b, stats)
    for step in range(2, count):
        lead_parts.append(shifted(columns(lead, step), "sp", step))
    down_mine = lax.dynamic_slice_in_dim(w_down, part * (depth // 2), depth // 2, 0)
    down_parts = [None] + [
        shifted(columns(down_mine, step), "sp", step) for step in range(1, count)
    ]
    hidden_a = head_outputs(
        query_a.reshape(tokens_dev, heads_dev, DKA),
        key_heads_a,
        value_heads_a,
        outgate_a,
        offset_a,
        carried_a,
        mstate[0],
        DKA,
    )
    hidden_b = head_outputs(
        query_b.reshape(tokens_dev, heads_dev, DKB),
        key_heads_b,
        value_heads_b,
        outgate_b,
        offset_b,
        carried_b,
        mstate[1],
        DKB,
    )
    hidden = jnp.stack([hidden_a, hidden_b], axis=1).reshape(tokens_dev, -1)
    proj_weight = out_proj.reshape(out_proj.shape[0], -1)
    row_block = hidden
    attn_rows = scatter_rows(
        lax.dot_general(
            row_block, proj_weight, (((1,), (1,)), ((), ())), preferred_element_type=jnp.float32
        )
    )
    resid_sum = resid.astype(jnp.float32) + attn_rows
    normed = (
        resid_sum
        * lax.rsqrt(jnp.mean(resid_sum * resid_sum, axis=1, keepdims=True) + EPS)
        * norm_gain
    )
    normed = normed.astype(jnp.bfloat16)
    pair_normed = swapped(normed, "sp")
    own = lambda weight: lax.dynamic_slice_in_dim(weight, side * half, half, 1)
    own_trail = jnp.where(part == 0, own(w_up), own(w_gate))
    lead_parts[0] = own(lead)
    trail_parts = [own_trail] + [side_swapped(piece) for piece in lead_parts[1:]]
    other_down = lax.dynamic_slice_in_dim(w_down, (1 - part) * (depth // 2), depth // 2, 0)
    down_parts[0] = own(down_mine)
    down_other = [own(other_down)] + [side_swapped(piece) for piece in down_parts[1:]]

    def placed(pieces, offset, blocks):
        whole = jnp.zeros((blocks * depth, half), jnp.bfloat16)
        for step, (first, second) in enumerate(pieces):
            origin = lax.rem(place - step + count, count) * depth
            whole = lax.dynamic_update_slice_in_dim(whole, first, origin + part * offset, 0)
            if second is not None:
                whole = lax.dynamic_update_slice_in_dim(
                    whole, second, origin + (1 - part) * offset, 0
                )
        return whole

    lead_full = placed([(piece, None) for piece in lead_parts], 0, count)
    trail_full = placed([(piece, None) for piece in trail_parts], 0, count)
    down_full = placed(list(zip(down_parts, down_other)), depth // 2, count)
    rows = jnp.concatenate([gather_rows(normed), gather_rows(pair_normed)])
    lead_act = jnp.dot(rows, lead_full, preferred_element_type=jnp.float32)
    trail_act = jnp.dot(rows, trail_full, preferred_element_type=jnp.float32)
    gate_act = jnp.where(part == 0, lead_act, trail_act)
    up_act = jnp.where(part == 0, trail_act, lead_act)
    inner_act = (jax.nn.silu(gate_act) * up_act).astype(jnp.bfloat16)
    partial = lax.dot_general(
        inner_act, down_full, (((1,), (1,)), ((), ())), preferred_element_type=jnp.float32
    ).astype(jnp.bfloat16)
    partial = partial.reshape(2, -1, partial.shape[-1])
    partial = jnp.stack([by_owner(partial[0]), by_owner(partial[1])])
    return (resid_sum + scatter_pair(partial)).astype(jnp.bfloat16)


MESH = pl.DeviceIdType.MESH
NT = (((1,), (1,)), ((), ()))
TN = (((0,), (0,)), ((), ()))
F32 = jnp.float32
BF16 = jnp.bfloat16
SUBS = 2
LAG_B, LAG_C, LAG_D, RING = 2, 5, 8, 8
VMEM_BYTES = 60 * 2**20


SENDS = (
    (((0, 1),), ((1, 1), (2, 1), (3, 1)), ((0, 2), (1, 2), (2, 2), (3, 2)), (), ((0, 3), (1, 3), (2, 3), (3, 3)), (), (), ((4, 1), (5, 1), (4, 3), (4, 2), (5, 3), (5, 2))),
    (((0, 0), (1, 0), (2, 0), (3, 0), (0, 2), (1, 2)), ((2, 2), (3, 2)), ((4, 2), (5, 2)), (), (), ((0, 3), (1, 3), (2, 3), (3, 3), (4, 3), (5, 3)), ((4, 0), (5, 0)), ()),
    (((0, 0), (0, 1), (1, 0), (1, 1), (2, 0), (2, 1), (3, 0), (3, 1), (4, 0), (4, 1), (5, 0), (5, 1), (0, 3), (1, 3), (4, 3)), ((2, 3), (3, 3), (5, 3)), (), (), (), (), (), ()),
    (((0, 0), (0, 1), (0, 2), (1, 0), (1, 1), (1, 2), (2, 0), (2, 1), (2, 2), (3, 0), (3, 1), (3, 2)), (), (), (), (), ((4, 2), (5, 2), (4, 0), (4, 1), (5, 0), (5, 1)), (), ()),
)
FORWARDS = (
    ((), ((0, 3),), ((0, 1), (0, 2), (1, 3), (1, 1)), ((2, 1), (2, 3), (3, 1), (1, 2)), ((3, 3), (2, 2)), (), ((3, 2),), ((4, 1),), ((4, 3),)),
    (((0, 0), (0, 3)), (), ((1, 0), (2, 0), (1, 3), (3, 0), (0, 2)), ((2, 3),), ((3, 3),), ((1, 2),), ((2, 2),), (), ((3, 2),)),
    (((0, 1), (1, 1), (0, 3)), (), ((2, 1), (1, 3)), ((0, 0), (1, 0), (2, 0), (2, 3), (3, 0), (3, 1), (4, 1)), ((3, 3),), (), ((4, 3), (5, 1), (5, 3)), (), ()),
    (((0, 2), (1, 2), (4, 2)), ((2, 2),), (), ((3, 2), (5, 2)), (), ((0, 0), (1, 0), (2, 0), (3, 0), (0, 1), (1, 1)), (), ((2, 1),), ((3, 1),)),
)
LATE = (
    ((), (), (), ((5, 1),), (), ((5, 3),), ((4, 2),), ((5, 2),)),
    ((), ((4, 3), (4, 0)), (), (), ((5, 3), (5, 0)), (), ((4, 2),), ((5, 2),)),
    ((), (), (), (), ((4, 0),), (), ((5, 0),), ()),
    ((), (), (), (), ((4, 1), (4, 0)), (), ((5, 0),), ((5, 1),)),
)
ROUNDS = (
    ((1, 0), (0, 0), (3, 0), (1, 1), (0, 1), (3, 1), (2, 0), (2, 1)),
    ((2, 0), (3, 0), (2, 1), (3, 1), (0, 0), (1, 0), (0, 1), (1, 1)),
)


def scan_lanes(value, combine, neutral):
    length = value.shape[1]
    lane = lax.broadcasted_iota(jnp.int32, value.shape, 1)
    step = 1
    while step < length:
        moved = jnp.where(lane >= step, pltpu.roll(value, step, 1), neutral)
        value = combine(value, moved)
        step *= 2
    return value


def fused_body(
    sizes,
    query_a,
    key_a,
    query_b,
    key_b,
    values_a,
    values_b,
    outgate_a,
    outgate_b,
    input_pre,
    forget_pre,
    resid,
    out_proj,
    gain,
    w_gate,
    w_up,
    w_down,
    out_ref,
    qa, ka, qb, kb, va, vb, oga, ogb, inp, fgt, res, proj, gn,
    wg, wu, wd,
    cols, offs, bstate, st_out, st_in, stat_out, stat_in, intra, hidden,
    part1, keep1, dsend1, drecv1, xsend1, xrecv1, rsum,
    rows, act, inner, part2, keep2, dsend2, drecv2, xsend2, xrecv2, zsend2, zrecv2,
    lsem, zs, zr, ys, yr, cs, cr, d1s, d1r, x1s, x1r, ags, agr,
    d2s, d2r, x2s, x2r, z2s, z2r,
):
    count, tokens, heads, depth, half, block, chunk1, _ = sizes
    g, s, t = lax.axis_index("grp"), lax.axis_index("sp"), lax.axis_index("tp")
    x, c = lax.div(t, 2), lax.rem(t, 2)
    core_peer = (g, s, t + 1 - 2 * c)
    x_peer = (g, s, t + 2 - 4 * x)
    y_peer = (1 - g, s, t)
    pair = (g, s + 1 - 2 * lax.rem(s, 2), t)
    part_rows = depth // 2
    sub_rows = part_rows // SUBS

    def remote(src, dst, send, recv, device):
        return pltpu.make_async_remote_copy(
            src_ref=src, dst_ref=dst, send_sem=send, recv_sem=recv,
            device_id=device, device_id_type=MESH,
        )

    barrier = pltpu.get_barrier_semaphore()
    for device in (core_peer, x_peer, y_peer):
        pl.semaphore_signal(barrier, inc=1, device_id=device, device_id_type=MESH)
    for place in range(count):
        @pl.when(place != s)
        def _():
            pl.semaphore_signal(barrier, inc=1, device_id=(g, place, t), device_id_type=MESH)

    side = lax.rem(s, 2)
    own_cols = pl.ds(pl.multiple_of(side * half, 128), half)
    own_rows = pl.ds(pl.multiple_of(s * depth, depth), depth)
    loads = [
        (input_pre, inp), (forget_pre, fgt), (key_a, ka), (key_b, kb), (values_a, va),
        (values_b, vb), (query_a, qa), (query_b, qb), (outgate_a, oga), (outgate_b, ogb),
        (out_proj, proj), (resid, res), (gain, gn),
        (w_gate.at[:, own_cols], wg.at[own_rows]),
        (w_up.at[:, own_cols], wu.at[own_rows]),
        (w_down.at[:, own_cols], wd.at[own_rows]),
    ]
    local = [pltpu.make_async_copy(a, b, lsem.at[i]) for i, (a, b) in enumerate(loads)]
    for copy in local[:8]:
        copy.start()

    whole_of = (wg,) * SUBS + (wu,) * SUBS + (wd,) * SUBS
    held_of = (w_gate,) * SUBS + (w_up,) * SUBS + (w_down,) * SUBS
    gates, ups, _ = (range(i * SUBS, (i + 1) * SUBS) for i in range(3))

    def piece_rows(pid, source, which):
        start = source * depth + which * part_rows + (pid % SUBS) * sub_rows
        return pl.ds(pl.multiple_of(start, sub_rows), sub_rows)

    def z_copy(pid, dest):
        start = g * part_rows + (pid % SUBS) * sub_rows
        src = held_of[pid].at[
            pl.ds(pl.multiple_of(start, sub_rows), sub_rows), pl.ds((dest % 2) * half, half)
        ]
        return remote(
            src, whole_of[pid].at[piece_rows(pid, s, g)],
            zs.at[pid, dest], zr.at[pid, s], (g, dest, t),
        )

    def y_copy(pid, source, which):
        place = whole_of[pid].at[piece_rows(pid, source, which)]
        return remote(place, place, ys.at[pid, source], yr.at[pid, source], y_peer)

    def arrived_z(pid, source):
        place = whole_of[pid].at[piece_rows(pid, source, g)]
        remote(place, place, zs.at[pid, source], zr.at[pid, source], y_peer).wait_recv()

    last = count - 1

    def issue(point):
        for place, plan in enumerate(SENDS):
            @pl.when(s == place)
            def _():
                for pid, dest in plan[point]:
                    z_copy(pid, dest).start()

    def hand_on(pieces):
        for pid, source in pieces:
            arrived_z(pid, source)
            y_copy(pid, source, g).start()

    def serve(point):
        for place, plan in enumerate(FORWARDS):
            @pl.when(s == place)
            def _():
                hand_on(plan[point])

    pl.semaphore_wait(barrier, 3 + count - 1)
    issue(0)

    for i in range(2):
        local[i].wait()
    quad = lambda ref: jnp.concatenate([ref[0], ref[1], ref[0], ref[1]], axis=0)
    raw_forget, raw_input = quad(fgt), quad(inp)
    log_forget = jnp.minimum(raw_forget, 0.0) - jnp.log1p(jnp.exp(-jnp.abs(raw_forget)))
    cum = scan_lanes(log_forget, lambda a, b: a + b, 0.0)
    offset = raw_input - cum
    run = scan_lanes(offset, jnp.maximum, NEG)
    fsum = cum[:, tokens - 1 : tokens]
    top = run[:, tokens - 1 : tokens]
    bmax = fsum + top
    decay = jnp.exp(offset - top)
    offs[...] = offset
    group = 2 * heads
    cols[...] = jnp.transpose(jnp.concatenate([decay[:group], run[:group]], axis=0))

    for i in range(2, 6):
        local[i].wait()
    head_lane = lax.div(lax.broadcasted_iota(jnp.int32, (tokens, heads * DKB), 1), DKB)
    state_of = []
    for h in range(heads):
        column = cols[:, h : h + 1]
        scaled = (ka[:, h * DKA : (h + 1) * DKA].astype(F32) * column).astype(BF16)
        state = lax.dot_general(
            scaled, va[:, h * DV : (h + 1) * DV], TN, preferred_element_type=F32
        )
        bstate[h * DKA : (h + 1) * DKA, :] = state
        state_of.append((h * DKA, DKA, h))
    base_b = heads * DKA
    for h in range(heads):
        column = cols[:, heads + h : heads + h + 1]
        scaled = (kb[...].astype(F32) * column).astype(BF16)
        state = lax.dot_general(
            scaled, vb[:, h * DV : (h + 1) * DV], TN, preferred_element_type=F32
        )
        bstate[base_b + h * DKB : base_b + (h + 1) * DKB, :] = state[h * DKB : (h + 1) * DKB]
        state_of.append((base_b + h * DKB, DKB, heads + h))

    after_peer = (g, jnp.minimum(s + 1, last), t)
    chain = [
        remote(
            st_out.at[pl.ds(start, size)], st_in.at[pl.ds(start, size)],
            cs.at[h], cr.at[h], after_peer,
        )
        for start, size, h in state_of
    ]
    chain_stat = remote(stat_out, stat_in, cs.at[group], cr.at[group], after_peer)
    wide = lambda row: jnp.concatenate([row] * (DV // 128), axis=1)

    def combine_stat():
        before = stat_in[...]
        total = before + fsum
        after = jnp.maximum(total, bmax)
        stat_out[...] = after
        chain_stat.start()
        return jnp.exp(total - after), jnp.exp(jnp.broadcast_to(bmax, total.shape) - after)

    def combine_head(i, keep_old, keep_new):
        start, size, h = state_of[i]
        st_out[start : start + size, :] = (
            wide(keep_old[h : h + 1, :]) * st_in[start : start + size, :].astype(F32)
            + wide(keep_new[h : h + 1, :]) * bstate[start : start + size, :]
        ).astype(BF16)
        chain[i].start()

    @pl.when(s == 0)
    def _():
        st_in[...] = jnp.zeros_like(st_in)
        stat_in[...] = jnp.full_like(stat_in, NEG)
        keeps = combine_stat()
        for i in range(group):
            combine_head(i, *keeps)
        issue(1)

    for copy in local[8:]:
        copy.start()
    for i in range(6, 8):
        local[i].wait()
    causal = lax.broadcasted_iota(jnp.int32, (tokens, tokens), 0) >= lax.broadcasted_iota(
        jnp.int32, (tokens, tokens), 1
    )

    def query_of(h):
        if h < heads:
            return qa[:, h * DKA : (h + 1) * DKA]
        return jnp.where(head_lane == h - heads, qb[...], jnp.zeros_like(qb[...]))

    for h in range(group):
        key = ka[:, h * DKA : (h + 1) * DKA] if h < heads else kb[...]
        value_ref, at = (va, h) if h < heads else (vb, h - heads)
        width = DKA if h < heads else DKB
        scores = lax.dot_general(query_of(h), key, NT, preferred_element_type=F32)
        exponent = jnp.where(causal, offs[h : h + 1, :] - cols[:, group + h : group + h + 1], NEG)
        weights = (scores * width ** (-0.5) * jnp.exp(exponent)).astype(BF16)
        intra[h] = jnp.dot(
            weights, value_ref[:, at * DV : (at + 1) * DV], preferred_element_type=F32
        )

    @pl.when(jnp.logical_and(s > 0, s < last))
    def _():
        chain_stat.wait_recv()
        keeps = combine_stat()
        for i in range(group):
            chain[i].wait_recv()
            combine_head(i, *keeps)
        issue(1)

    @pl.when(s == last)
    def _():
        chain_stat.wait_recv()
        for copy in chain:
            copy.wait_recv()

    serve(0)
    for i in range(8, 10):
        local[i].wait()
    for h in range(group):
        width = DKA if h < heads else DKB
        gate_ref, at = (oga, h) if h < heads else (ogb, h - heads)
        state = (
            st_in[h * DKA : (h + 1) * DKA, :] if h < heads else st_in[base_b:, :]
        )
        entering_max = stat_in[h : h + 1, 0:1]
        own_max = cols[:, group + h : group + h + 1]
        top_max = jnp.maximum(own_max, entering_max)
        carried = jnp.dot(query_of(h), state, preferred_element_type=F32)
        numer = carried * (width ** (-0.5) * jnp.exp(entering_max - top_max)) + intra[
            h
        ] * jnp.exp(own_max - top_max)
        inv = lax.rsqrt(jnp.mean(numer * numer, axis=1, keepdims=True) + EPS)
        gated = numer * inv * jax.nn.sigmoid(gate_ref[:, at * DV : (at + 1) * DV].astype(F32))
        hidden[:, h * DV : (h + 1) * DV] = gated.astype(BF16)

    serve(1)

    for i in range(10, 13):
        local[i].wait()
    chunks1 = proj.shape[0] // chunk1

    def block_rows(chip, core):
        return pl.ds(pl.multiple_of((2 * chip + core) * block, 8), block)

    def d1(j):
        return remote(dsend1.at[j], drecv1.at[j], d1s.at[j], d1r.at[j], core_peer)

    def x1(j):
        return remote(xsend1.at[j], xrecv1.at[j], x1s.at[j], x1r.at[j], x_peer)

    def attn_step(j, carry):
        @pl.when(j < chunks1)
        def _():
            weight = proj[pl.ds(pl.multiple_of(j * chunk1, chunk1), chunk1)]
            part1[...] = lax.dot_general(
                hidden[...], weight.reshape(chunk1, hidden.shape[1]), NT,
                preferred_element_type=F32,
            )
            for role in range(2):
                chip = x if role == 0 else 1 - x
                dsend1[j, role] = part1[block_rows(chip, 1 - c)].astype(BF16)
                keep1[j, role] = part1[block_rows(chip, c)]
            d1(j).start()

        @pl.when(j >= 1)
        def _():
            k = j - 1
            d1(k).wait_recv()
            xsend1[k] = (keep1[k, 1] + drecv1[k, 1].astype(F32)).astype(BF16)
            x1(k).start()
            keep1[k, 0] = keep1[k, 0] + drecv1[k, 0].astype(F32)

        return carry

    lax.fori_loop(0, chunks1 + 1, attn_step, 0)
    issue(2)
    serve(2)
    for j in range(chunks1):
        span = slice(j * chunk1, (j + 1) * chunk1)
        x1(j).wait_recv()
        rsum[:, span] = res[:, span].astype(F32) + keep1[j, 0] + xrecv1[j].astype(F32)
    summed = rsum[...]
    scale = lax.rsqrt(jnp.mean(summed * summed, axis=1, keepdims=True) + EPS)
    mine = block_rows(x, c)
    rows[0, mine] = (summed * scale * gn[...]).astype(BF16)

    def move(kind, src_place, dst_place, chip, core, device):
        return remote(
            rows.at[src_place, block_rows(chip, core)],
            rows.at[dst_place, block_rows(chip, core)],
            ags.at[kind], agr.at[kind], device,
        )

    own_z = move(2, 0, 1, x, c, pair)
    own_x = move(1, 0, 0, x, c, x_peer)
    own_d = move(0, 0, 0, x, c, core_peer)
    own_z.start()
    own_x.start()
    own_d.start()
    issue(3)

    def arrived(kind, place, chip, core):
        move(kind, place, place, chip, core, core_peer).wait_recv()

    serve(3)
    issue(4)
    arrived(1, 0, 1 - x, c)
    fwd_x = move(3, 0, 0, 1 - x, c, core_peer)
    fwd_x.start()
    serve(4)
    arrived(2, 1, x, c)
    fwd_zx = move(5, 1, 1, x, c, x_peer)
    fwd_zd = move(4, 1, 1, x, c, core_peer)
    fwd_zx.start()
    fwd_zd.start()
    issue(5)
    serve(5)

    def take_y(pids):
        for place in range(count):
            @pl.when(place != s)
            def _():
                for pid in pids:
                    y_copy(pid, place, 1 - g).wait_recv()

    for i in range(13, 16):
        local[i].wait()
    take_y(gates)
    arrived(0, 0, x, 1 - c)
    arrived(3, 0, 1 - x, 1 - c)
    act[0] = jnp.dot(rows[0], wg[...], preferred_element_type=F32)
    serve(6)
    arrived(5, 1, 1 - x, c)
    issue(6)
    fwd_xd = move(6, 1, 1, 1 - x, c, core_peer)
    fwd_xd.start()
    serve(7)
    arrived(4, 1, x, 1 - c)
    arrived(6, 1, 1 - x, 1 - c)
    act[1] = jnp.dot(rows[1], wg[...], preferred_element_type=F32)
    serve(8)
    take_y(ups)

    def up_step(p, carry):
        gate = act[p]
        up = jnp.dot(rows[p], wu[...], preferred_element_type=F32)
        start = pl.multiple_of(p * tokens, tokens)
        inner[pl.ds(start, tokens), :] = (gate / (1.0 + jnp.exp(-gate)) * up).astype(BF16)
        return carry

    lax.fori_loop(0, 2, up_step, 0)
    issue(7)

    rounds = count * SUBS
    chunks2 = 2 * rounds

    def look(table, k):
        value = jnp.int32(table[0])
        for i, entry in enumerate(table[1:], 1):
            value = jnp.where(k == i, entry, value)
        return value

    low = s < count // 2

    def place_of(p):
        is_y = jnp.logical_or(
            jnp.logical_and(p > 0, lax.rem(p, 2) == 0), p == chunks2 - 1
        )
        r = jnp.where(
            p == chunks2 - 1, rounds - 1,
            jnp.where(is_y, lax.div(p, 2) - 1, lax.div(p + 1, 2)),
        )
        r = jnp.maximum(r, 0)
        b, sub = (
            jnp.where(low, *(look([pick[i] for pick in order], r) for order in ROUNDS))
            for i in range(2)
        )
        which = jnp.where(is_y, 1 - g, g)
        return b, sub, which, is_y, r

    def down_rows(p):
        b, sub, which, _, _ = place_of(p)
        return b * depth + which * part_rows + sub * sub_rows

    def d2(k):
        return remote(dsend2.at[k], drecv2.at[k], d2s.at[k], d2r.at[k], core_peer)

    def x2(k):
        return remote(xsend2.at[k], xrecv2.at[k], x2s.at[k], x2r.at[k], x_peer)

    def z2(k):
        return remote(zsend2.at[k], zrecv2.at[k], z2s.at[k], z2r.at[k], pair)

    def down_step(p, carry):
        @pl.when(p < chunks2)
        def _():
            b, sub, _, is_y, r = place_of(p)
            start = pl.multiple_of(down_rows(p), sub_rows)
            spot = wd.at[pl.ds(start, sub_rows)]
            pid = 2 * SUBS + sub
            y_both = remote(spot, spot, ys.at[pid, b], yr.at[pid, b], y_peer)

            for place, plan in enumerate(LATE):
                for k, pieces in enumerate(plan):
                    if pieces:
                        now = jnp.logical_and(s == place, r == k)

                        @pl.when(jnp.logical_and(now, jnp.logical_not(is_y)))
                        def _():
                            hand_on(pieces)

            @pl.when(jnp.logical_and(b != s, is_y))
            def _():
                y_both.wait_recv()

            part2[...] = lax.dot_general(
                inner[...], wd[pl.ds(start, sub_rows), :], NT, preferred_element_type=F32
            )
            ring = lax.rem(p, RING)
            for place in range(2):
                for role in range(2):
                    chip = x if role == 0 else 1 - x
                    send = pl.multiple_of(place * tokens + (2 * chip + 1 - c) * block, 8)
                    hold = pl.multiple_of(place * tokens + (2 * chip + c) * block, 8)
                    dsend2[p, 2 * place + role] = part2[pl.ds(send, block)].astype(BF16)
                    keep2[ring, 2 * place + role] = part2[pl.ds(hold, block)]
            d2(p).start()

        @pl.when(jnp.logical_and(p >= LAG_B, p < chunks2 + LAG_B))
        def _():
            k = p - LAG_B
            ring = lax.rem(k, RING)
            d2(k).wait_recv()
            for place in range(2):
                xsend2[k, place] = (
                    keep2[ring, 2 * place + 1] + drecv2[k, 2 * place + 1].astype(F32)
                ).astype(BF16)
            x2(k).start()
            for place in range(2):
                keep2[ring, 2 * place] = keep2[ring, 2 * place] + drecv2[
                    k, 2 * place
                ].astype(F32)

        @pl.when(jnp.logical_and(p >= LAG_C, p < chunks2 + LAG_C))
        def _():
            k = p - LAG_C
            ring = lax.rem(k, RING)
            x2(k).wait_recv()
            zsend2[k] = (keep2[ring, 2] + xrecv2[k, 1].astype(F32)).astype(BF16)
            z2(k).start()
            span = pl.ds(pl.multiple_of(down_rows(k), sub_rows), sub_rows)
            rsum[:, span] = rsum[:, span] + keep2[ring, 0] + xrecv2[k, 0].astype(F32)

        @pl.when(p >= LAG_D)
        def _():
            k = p - LAG_D
            z2(k).wait_recv()
            span = pl.ds(pl.multiple_of(down_rows(k), sub_rows), sub_rows)
            out_ref[:, span] = (rsum[:, span] + zrecv2[k].astype(F32)).astype(BF16)

        return carry

    lax.fori_loop(0, chunks2 + LAG_D, down_step, 0)

    for pid in range(3 * SUBS):
        for dest in range(count):
            @pl.when(dest != s)
            def _():
                z_copy(pid, dest).wait_send()
                y_copy(pid, dest, g).wait_send()

    @pl.when(s < last)
    def _():
        chain_stat.wait_send()
        for copy in chain:
            copy.wait_send()

    for copy in (own_z, own_x, own_d, fwd_x, fwd_zx, fwd_zd, fwd_xd):
        copy.wait_send()
    for j in range(chunks1):
        d1(j).wait_send()
        x1(j).wait_send()

    def drain(k, carry):
        d2(k).wait_send()
        x2(k).wait_send()
        z2(k).wait_send()
        return carry

    lax.fori_loop(0, chunks2, drain, 0)


def fused(*args):
    query_a, _, _, _, _ = args[:5]
    resid, w_gate = args[10], args[13]
    count = lax.axis_size("sp")
    tokens = query_a.shape[0]
    heads = query_a.shape[1] // DKA
    depth, units = w_gate.shape
    half = units // 2
    block, width = resid.shape
    chunk1 = width // 4
    chunk2 = depth // 2 // SUBS
    chunks1, chunks2 = width // chunk1, width // chunk2
    group = 2 * heads
    state_rows = heads * (DKA + DKB)
    sizes = (count, tokens, heads, depth, half, block, chunk1, chunk2)
    args = list(args)
    args[12] = args[12].reshape(1, width)
    vmem = lambda *shape, kind=BF16: pltpu.VMEM(shape, kind)
    dma = pltpu.SemaphoreType.DMA
    pieces = (3 * SUBS, count)
    copies = [args[i] for i in (0, 1, 2, 3, 4, 5, 6, 7, 8, 9, 10, 11, 12)]
    scratch = [pltpu.VMEM(a.shape, a.dtype) for a in copies]
    scratch += [vmem(width, half), vmem(width, half), vmem(width, half)]
    scratch += [
        vmem(tokens, 2 * group, kind=F32),
        vmem(2 * group, tokens, kind=F32),
        vmem(state_rows, DV, kind=F32),
        vmem(state_rows, DV),
        vmem(state_rows, DV),
        vmem(2 * group, 128, kind=F32),
        vmem(2 * group, 128, kind=F32),
        vmem(group, tokens, DV, kind=F32),
        vmem(tokens, group * DV),
        vmem(tokens, chunk1, kind=F32),
        vmem(chunks1, 2, block, chunk1, kind=F32),
        vmem(chunks1, 2, block, chunk1),
        vmem(chunks1, 2, block, chunk1),
        vmem(chunks1, block, chunk1),
        vmem(chunks1, block, chunk1),
        vmem(block, width, kind=F32),
        vmem(2, tokens, width),
        vmem(2, tokens, half, kind=F32),
        vmem(2 * tokens, half),
        vmem(2 * tokens, chunk2, kind=F32),
        vmem(RING, 4, block, chunk2, kind=F32),
        vmem(chunks2, 4, block, chunk2),
        vmem(chunks2, 4, block, chunk2),
        vmem(chunks2, 2, block, chunk2),
        vmem(chunks2, 2, block, chunk2),
        vmem(chunks2, block, chunk2),
        vmem(chunks2, block, chunk2),
    ]
    scratch += [dma((16,)), dma(pieces), dma(pieces), dma(pieces), dma(pieces), dma((group + 1,)), dma((group + 1,))]
    scratch += [dma((chunks1,))] * 4 + [dma((7,))] * 2 + [dma((chunks2,))] * 6
    return pl.pallas_call(
        functools.partial(fused_body, sizes),
        out_shape=jax.ShapeDtypeStruct(resid.shape, BF16),
        in_specs=[pl.BlockSpec(memory_space=pl.ANY)] * len(args),
        out_specs=pl.BlockSpec(memory_space=pltpu.VMEM),
        scratch_shapes=scratch,
        compiler_params=pltpu.CompilerParams(
            collective_id=0, has_side_effects=True, vmem_limit_bytes=VMEM_BYTES
        ),
    )(*args)


def layer(*args):
    return local(*args)


def solution(mesh):
    few = mesh.shape["sp"] == 4 and mesh.shape["tp"] == 4
    return jax.shard_map(
        fused if few else layer,
        mesh=mesh,
        in_specs=(
            P(("grp", "sp"), "tp"),
            P(("grp", "sp"), "tp"),
            P(("grp", "sp"), "tp"),
            P(("grp", "sp"), "tp"),
            P(("grp", "sp"), "tp"),
            P(("grp", "sp"), "tp"),
            P(("grp", "sp"), "tp"),
            P(("grp", "sp"), "tp"),
            P(None, "tp", ("grp", "sp")),
            P(None, "tp", ("grp", "sp")),
            P(("grp", "sp", "tp"), None),
            P(None, None, "tp"),
            P(),
            P("sp", "tp"),
            P("sp", "tp"),
            P("sp", "tp"),
        ),
        out_specs=P(("grp", "sp", "tp"), None),
        check_vma=False,
    )
```

```python
import functools

import jax
import jax.numpy as jnp
from jax import lax
from jax.experimental import pallas as pl
from jax.experimental.pallas import tpu as pltpu
from jax.sharding import PartitionSpec as P

DKA = 128
DKB = 64
DV = 256


EPS = 1e-06
NEG = -1e30


def summarize(key_heads, value_head_rows, input_log, forget_raw):
    cum_forget = jnp.cumsum(jax.nn.log_sigmoid(forget_raw), axis=1)
    offset_log = input_log - cum_forget
    block_sum = cum_forget[:, -1]
    block_max = block_sum + jnp.max(offset_log, axis=1)
    key_decay = jnp.exp(block_sum[:, None] + offset_log - block_max[:, None])
    scaled_keys = (key_heads.astype(jnp.float32) * jnp.transpose(key_decay)[:, :, None]).astype(
        jnp.bfloat16
    )
    block_memory_state = jnp.einsum(
        "eif,eiw->ifw", scaled_keys, value_head_rows, preferred_element_type=jnp.float32
    )
    return (block_memory_state, block_max, block_sum, offset_log)


def head_outputs(
    query_head_rows,
    key_heads,
    value_head_rows,
    outgate,
    offset_log,
    carried_over,
    mstate,
    key_width,
):
    length = query_head_rows.shape[0]
    run_max = jnp.maximum(lax.cummax(offset_log, axis=1), mstate[:, None])
    causal = jnp.arange(length)[:, None] >= jnp.arange(length)[None, :]
    exponent = jnp.where(causal[None], offset_log[:, None, :] - run_max[:, :, None], -jnp.inf)
    scores = jnp.einsum(
        "thk,shk->hts", query_head_rows, key_heads, preferred_element_type=jnp.float32
    )
    scores = scores * key_width ** (-0.5) * jnp.exp(exponent)
    weights_bf = scores.astype(jnp.bfloat16)
    inner_part = jnp.einsum(
        "hts,shv->thv", weights_bf, value_head_rows, preferred_element_type=jnp.float32
    )
    carried_portion = jnp.einsum(
        "pix,ixe->pie",
        query_head_rows,
        carried_over.astype(jnp.bfloat16),
        preferred_element_type=jnp.float32,
    ) * key_width ** (-0.5)
    carried_portion = (
        carried_portion * jnp.transpose(jnp.exp(mstate[:, None] - run_max))[:, :, None]
    )
    numerator = carried_portion + inner_part
    inv_rms = lax.rsqrt(jnp.mean(numerator * numerator, axis=2, keepdims=True) + EPS)
    gated_out = (
        numerator * inv_rms * jax.nn.sigmoid(outgate.astype(jnp.float32).reshape(numerator.shape))
    )
    return gated_out.reshape(length, -1).astype(jnp.bfloat16)


def shifted(value, axis, shift):
    count = lax.axis_size(axis)
    return lax.ppermute(value, axis, [(i, (i + shift) % count) for i in range(count)])


def swapped(value, axis):
    count = lax.axis_size(axis)
    return lax.ppermute(value, axis, [(i, i ^ 1) for i in range(count)])


def side_swapped(value):
    return swapped(value, "grp")


def column_shifted(value, shift):
    count = lax.axis_size("tp")
    return lax.ppermute(value, "tp", [(i, (i + 2 * shift) % count) for i in range(count)])


def split_wide(value):
    high = lax.reduce_precision(value, 8, 7)
    middle = lax.reduce_precision(value - high, 8, 7)
    return jnp.stack([high, middle, value - high - middle]).astype(jnp.bfloat16)


def entering(state_a, state_b, stats):
    count, mine = lax.axis_size("sp"), lax.axis_index("sp")
    heads, depth_a, width = state_a.shape
    depth_b = state_b.shape[1]
    terms = split_wide(stats).transpose(3, 0, 1, 2).reshape(heads, 1, 12)
    terms = jnp.pad(terms, ((0, 0), (0, 15), (0, width - 12)))
    packed = jnp.concatenate(
        [state_a.astype(jnp.bfloat16), state_b.astype(jnp.bfloat16), terms], axis=1
    )
    parts = [
        lax.ppermute(packed, "sp", [(i, i + step) for i in range(count - step)])
        for step in range(1, count)
    ]
    total = jnp.zeros_like(stats[1])
    highest = jnp.full_like(stats[0], NEG)
    logs = []
    for step in range(1, count):
        got = parts[step - 1][:, depth_a + depth_b, :12].astype(jnp.float32)
        stat = jnp.sum(got.reshape(heads, 3, 2, 2), axis=1).transpose(1, 2, 0)
        logs.append(jnp.where(step <= mine, stat[0] + total, NEG))
        total = total + stat[1]
        highest = jnp.maximum(highest, logs[-1])
    carried_a, carried_b = jnp.zeros_like(state_a), jnp.zeros_like(state_b)
    for step in range(1, count):
        weight = jnp.where(step <= mine, jnp.exp(logs[step - 1] - highest), 0.0)[:, :, None, None]
        part = parts[step - 1].astype(jnp.float32)
        carried_a += weight[0] * part[:, :depth_a]
        carried_b += weight[1] * part[:, depth_a : depth_a + depth_b]
    return carried_a, carried_b, highest


def scatter_pair(partial):
    chips = lax.axis_size("tp") // 2
    me = lax.axis_index("tp")
    chip, core = me // 2, me % 2
    parts = partial.reshape(2, chips, 2, -1, partial.shape[-1])
    away = lax.dynamic_index_in_dim(parts, 1 - core, 2, keepdims=False).astype(jnp.bfloat16)
    kept = lax.dynamic_index_in_dim(parts, core, 2, keepdims=False)
    got = swapped(away, "tp")
    totals = []
    for which in (1, 0):
        both = kept[which].astype(jnp.float32) + got[which].astype(jnp.float32)
        total = lax.dynamic_index_in_dim(both, chip, 0, keepdims=False)
        for step in range(1, chips):
            target = lax.rem(chip + step, chips)
            sent = lax.dynamic_index_in_dim(both, target, 0, keepdims=False).astype(jnp.bfloat16)
            total = total + column_shifted(sent, step).astype(jnp.float32)
        totals.append(total)
    return totals[1] + swapped(totals[0].astype(jnp.bfloat16), "sp").astype(jnp.float32)


def scatter_rows(partial):
    chips = lax.axis_size("tp") // 2
    me = lax.axis_index("tp")
    chip, core = me // 2, me % 2
    parts = partial.reshape(chips, 2, -1, partial.shape[-1])
    away = lax.dynamic_index_in_dim(parts, 1 - core, 1, keepdims=False).astype(jnp.bfloat16)
    kept = lax.dynamic_index_in_dim(parts, core, 1, keepdims=False)
    both = kept.astype(jnp.float32) + swapped(away, "tp").astype(jnp.float32)
    total = lax.dynamic_index_in_dim(both, chip, 0, keepdims=False)
    for step in range(1, chips):
        target = lax.rem(chip + step, chips)
        sent = lax.dynamic_index_in_dim(both, target, 0, keepdims=False).astype(jnp.bfloat16)
        total = total + column_shifted(sent, step).astype(jnp.float32)
    return total


def gather_rows(rows):
    chips = lax.axis_size("tp") // 2
    core = lax.axis_index("tp") % 2
    mine = jnp.stack([rows] + [column_shifted(rows, step) for step in range(1, chips)])
    other = swapped(mine, "tp")
    first = jnp.where(core == 0, mine, other)
    second = jnp.where(core == 0, other, mine)
    gathered = jnp.stack([first, second], axis=1)
    return gathered.reshape(-1, rows.shape[-1])


def by_owner(partial):
    chips = lax.axis_size("tp") // 2
    chip = lax.axis_index("tp") // 2
    parts = partial.reshape(chips, -1, partial.shape[-1])
    order = [
        lax.dynamic_index_in_dim(parts, lax.rem(chip - owner + chips, chips), 0)
        for owner in range(chips)
    ]
    return jnp.concatenate(order).reshape(partial.shape)


def local(
    query_a,
    key_a,
    query_b,
    key_b,
    values_a,
    values_b,
    outgate_a,
    outgate_b,
    input_pre,
    forget_pre,
    resid,
    out_proj,
    norm_gain,
    w_gate,
    w_up,
    w_down,
):
    tokens_dev = query_a.shape[0]
    heads_dev = query_a.shape[1] // DKA
    count, place, part = lax.axis_size("sp"), lax.axis_index("sp"), lax.axis_index("grp")
    depth, units = w_gate.shape
    half = units // 2
    side = lax.rem(place, 2)

    def columns(weight, step):
        target_side = lax.rem(place + step, 2)
        return lax.dynamic_slice_in_dim(weight, target_side * half, half, 1)

    lead = jnp.where(part == 0, w_gate, w_up)
    first_sent = columns(lead, 1)
    lead_parts = [None, shifted(first_sent, "sp", 1)]
    key_heads_a = key_a.reshape(tokens_dev, heads_dev, DKA)
    key_heads_b = key_b.reshape(tokens_dev, heads_dev, DKB)
    value_heads_a = values_a.reshape(tokens_dev, heads_dev, DV)
    value_heads_b = values_b.reshape(tokens_dev, heads_dev, DV)
    state_a, max_a, sum_a, offset_a = summarize(
        key_heads_a, value_heads_a, input_pre[0], forget_pre[0]
    )
    state_b, max_b, sum_b, offset_b = summarize(
        key_heads_b, value_heads_b, input_pre[1], forget_pre[1]
    )
    stats = jnp.stack([jnp.stack([max_a, max_b]), jnp.stack([sum_a, sum_b])])
    lead, w_down, state_a, state_b, stats = lax.optimization_barrier(
        (lead, w_down, state_a, state_b, stats)
    )
    carried_a, carried_b, mstate = entering(state_a, state_b, stats)
    for step in range(2, count):
        lead_parts.append(shifted(columns(lead, step), "sp", step))
    down_mine = lax.dynamic_slice_in_dim(w_down, part * (depth // 2), depth // 2, 0)
    down_parts = [None] + [
        shifted(columns(down_mine, step), "sp", step) for step in range(1, count)
    ]
    hidden_a = head_outputs(
        query_a.reshape(tokens_dev, heads_dev, DKA),
        key_heads_a,
        value_heads_a,
        outgate_a,
        offset_a,
        carried_a,
        mstate[0],
        DKA,
    )
    hidden_b = head_outputs(
        query_b.reshape(tokens_dev, heads_dev, DKB),
        key_heads_b,
        value_heads_b,
        outgate_b,
        offset_b,
        carried_b,
        mstate[1],
        DKB,
    )
    hidden = jnp.stack([hidden_a, hidden_b], axis=1).reshape(tokens_dev, -1)
    proj_weight = out_proj.reshape(out_proj.shape[0], -1)
    row_block = hidden
    attn_rows = scatter_rows(
        lax.dot_general(
            row_block, proj_weight, (((1,), (1,)), ((), ())), preferred_element_type=jnp.float32
        )
    )
    resid_sum = resid.astype(jnp.float32) + attn_rows
    normed = (
        resid_sum
        * lax.rsqrt(jnp.mean(resid_sum * resid_sum, axis=1, keepdims=True) + EPS)
        * norm_gain
    )
    normed = normed.astype(jnp.bfloat16)
    pair_normed = swapped(normed, "sp")
    own = lambda weight: lax.dynamic_slice_in_dim(weight, side * half, half, 1)
    own_trail = jnp.where(part == 0, own(w_up), own(w_gate))
    lead_parts[0] = own(lead)
    trail_parts = [own_trail] + [side_swapped(piece) for piece in lead_parts[1:]]
    other_down = lax.dynamic_slice_in_dim(w_down, (1 - part) * (depth // 2), depth // 2, 0)
    down_parts[0] = own(down_mine)
    down_other = [own(other_down)] + [side_swapped(piece) for piece in down_parts[1:]]

    def placed(pieces, offset, blocks):
        whole = jnp.zeros((blocks * depth, half), jnp.bfloat16)
        for step, (first, second) in enumerate(pieces):
            origin = lax.rem(place - step + count, count) * depth
            whole = lax.dynamic_update_slice_in_dim(whole, first, origin + part * offset, 0)
            if second is not None:
                whole = lax.dynamic_update_slice_in_dim(
                    whole, second, origin + (1 - part) * offset, 0
                )
        return whole

    lead_full = placed([(piece, None) for piece in lead_parts], 0, count)
    trail_full = placed([(piece, None) for piece in trail_parts], 0, count)
    down_full = placed(list(zip(down_parts, down_other)), depth // 2, count)
    rows = jnp.concatenate([gather_rows(normed), gather_rows(pair_normed)])
    lead_act = jnp.dot(rows, lead_full, preferred_element_type=jnp.float32)
    trail_act = jnp.dot(rows, trail_full, preferred_element_type=jnp.float32)
    gate_act = jnp.where(part == 0, lead_act, trail_act)
    up_act = jnp.where(part == 0, trail_act, lead_act)
    inner_act = (jax.nn.silu(gate_act) * up_act).astype(jnp.bfloat16)
    partial = lax.dot_general(
        inner_act, down_full, (((1,), (1,)), ((), ())), preferred_element_type=jnp.float32
    ).astype(jnp.bfloat16)
    partial = partial.reshape(2, -1, partial.shape[-1])
    partial = jnp.stack([by_owner(partial[0]), by_owner(partial[1])])
    return (resid_sum + scatter_pair(partial)).astype(jnp.bfloat16)


MESH = pl.DeviceIdType.MESH
NT = (((1,), (1,)), ((), ()))
TN = (((0,), (0,)), ((), ()))
F32 = jnp.float32
BF16 = jnp.bfloat16
SUBS = 2
LAG_B, LAG_C, RING = 2, 5, 8
VMEM_BYTES = 60 * 2**20


SENDS = (
    (((0, 1),), ((1, 1), (2, 1), (3, 1)), ((0, 2), (1, 2), (2, 2), (3, 2)), (), ((0, 3), (1, 3), (2, 3), (3, 3)), (), (), ((4, 1), (5, 1), (4, 3), (4, 2), (5, 3), (5, 2))),
    (((0, 0), (1, 0), (2, 0), (3, 0), (0, 2), (1, 2)), ((2, 2), (3, 2)), ((4, 2), (5, 2)), (), (), ((0, 3), (1, 3), (2, 3), (3, 3), (4, 3), (5, 3)), ((4, 0), (5, 0)), ()),
    (((0, 0), (0, 1), (1, 0), (1, 1), (2, 0), (2, 1), (3, 0), (3, 1), (4, 0), (4, 1), (5, 0), (5, 1), (0, 3), (1, 3), (4, 3)), ((2, 3), (3, 3), (5, 3)), (), (), (), (), (), ()),
    (((0, 0), (0, 1), (0, 2), (1, 0), (1, 1), (1, 2), (2, 0), (2, 1), (2, 2), (3, 0), (3, 1), (3, 2)), (), (), (), (), ((4, 2), (5, 2), (4, 0), (4, 1), (5, 0), (5, 1)), (), ()),
)
FORWARDS = (
    ((), ((0, 3),), ((0, 1), (0, 2), (1, 3), (1, 1)), ((2, 1), (2, 3), (3, 1), (1, 2)), ((3, 3), (2, 2)), (), ((3, 2),), (), ()),
    (((0, 0), (0, 3)), (), ((1, 0), (2, 0), (1, 3), (3, 0), (0, 2)), ((2, 3),), ((3, 3),), ((1, 2),), ((2, 2),), (), ((3, 2),)),
    (((0, 1), (1, 1), (0, 3)), (), ((2, 1), (1, 3)), ((0, 0), (1, 0), (2, 0), (2, 3), (3, 0), (3, 1), (4, 1)), ((3, 3),), (), ((4, 3), (5, 1), (5, 3)), (), ()),
    (((0, 2), (1, 2), (4, 2)), ((2, 2),), (), ((3, 2), (5, 2)), (), ((0, 0), (1, 0), (2, 0), (3, 0), (0, 1), (1, 1), (2, 1)), (), (), ((3, 1),)),
)
LATE = (
    (((4, 1), (4, 3)), ((5, 1),), (), ((5, 3),), (), (), ((4, 2),), ((5, 2),)),
    ((), ((4, 3), (4, 0)), (), ((5, 3), (5, 0)), (), (), ((4, 2),), ((5, 2),)),
    ((), (), (), (), ((4, 0),), (), ((5, 0),), ()),
    (((4, 0),), (), ((5, 0),), (), ((4, 1),), (), ((5, 1),), ()),
)
ROUNDS = (
    ((1, 0), (0, 0), (3, 0), (1, 1), (0, 1), (3, 1), (2, 0), (2, 1)),
    ((2, 0), (3, 0), (2, 1), (3, 1), (0, 0), (1, 0), (0, 1), (1, 1)),
)


def scan_lanes(value, combine, neutral):
    length = value.shape[1]
    lane = lax.broadcasted_iota(jnp.int32, value.shape, 1)
    step = 1
    while step < length:
        moved = jnp.where(lane >= step, pltpu.roll(value, step, 1), neutral)
        value = combine(value, moved)
        step *= 2
    return value


def fused_body(
    sizes,
    query_a,
    key_a,
    query_b,
    key_b,
    values_a,
    values_b,
    outgate_a,
    outgate_b,
    input_pre,
    forget_pre,
    resid,
    out_proj,
    gain,
    w_gate,
    w_up,
    w_down,
    out_ref,
    qa, ka, qb, kb, va, vb, oga, ogb, inp, fgt, res, proj, gn,
    wg, wu, wd,
    cols, offs, bstate, st_out, st_in, stat_out, stat_in, intra, hidden,
    part1, keep1, dsend1, drecv1, xsend1, xrecv1, rsum,
    rows, act, inner, part2, keep2, dsend2, drecv2, xsend2, xrecv2, zsend2, zrecv2,
    lsem, zs, zr, ys, yr, cs, cr, d1s, d1r, x1s, x1r, ags, agr,
    d2s, d2r, x2s, x2r, z2s, z2r,
):
    count, tokens, heads, depth, half, block, chunk1, _ = sizes
    g, s, t = lax.axis_index("grp"), lax.axis_index("sp"), lax.axis_index("tp")
    x, c = lax.div(t, 2), lax.rem(t, 2)
    core_peer = (g, s, t + 1 - 2 * c)
    x_peer = (g, s, t + 2 - 4 * x)
    y_peer = (1 - g, s, t)
    pair = (g, s + 1 - 2 * lax.rem(s, 2), t)
    part_rows = depth // 2
    sub_rows = part_rows // SUBS

    def remote(src, dst, send, recv, device):
        return pltpu.make_async_remote_copy(
            src_ref=src, dst_ref=dst, send_sem=send, recv_sem=recv,
            device_id=device, device_id_type=MESH,
        )

    barrier = pltpu.get_barrier_semaphore()
    for device in (core_peer, x_peer, y_peer):
        pl.semaphore_signal(barrier, inc=1, device_id=device, device_id_type=MESH)
    for place in range(count):
        @pl.when(place != s)
        def _():
            pl.semaphore_signal(barrier, inc=1, device_id=(g, place, t), device_id_type=MESH)

    side = lax.rem(s, 2)
    own_cols = pl.ds(pl.multiple_of(side * half, 128), half)
    own_rows = pl.ds(pl.multiple_of(s * depth, depth), depth)
    loads = [
        (input_pre, inp), (forget_pre, fgt), (key_a, ka), (key_b, kb), (values_a, va),
        (values_b, vb), (query_a, qa), (query_b, qb), (outgate_a, oga), (outgate_b, ogb),
        (out_proj, proj), (resid, res), (gain, gn),
        (w_gate.at[:, own_cols], wg.at[own_rows]),
        (w_up.at[:, own_cols], wu.at[own_rows]),
        (w_down.at[:, own_cols], wd.at[own_rows]),
    ]
    local = [pltpu.make_async_copy(a, b, lsem.at[i]) for i, (a, b) in enumerate(loads)]
    for copy in local[:8]:
        copy.start()

    whole_of = (wg,) * SUBS + (wu,) * SUBS + (wd,) * SUBS
    held_of = (w_gate,) * SUBS + (w_up,) * SUBS + (w_down,) * SUBS
    gates, ups, _ = (range(i * SUBS, (i + 1) * SUBS) for i in range(3))

    def piece_rows(pid, source, which):
        start = source * depth + which * part_rows + (pid % SUBS) * sub_rows
        return pl.ds(pl.multiple_of(start, sub_rows), sub_rows)

    def z_copy(pid, dest):
        start = g * part_rows + (pid % SUBS) * sub_rows
        src = held_of[pid].at[
            pl.ds(pl.multiple_of(start, sub_rows), sub_rows), pl.ds((dest % 2) * half, half)
        ]
        return remote(
            src, whole_of[pid].at[piece_rows(pid, s, g)],
            zs.at[pid, dest], zr.at[pid, s], (g, dest, t),
        )

    def y_copy(pid, source, which):
        place = whole_of[pid].at[piece_rows(pid, source, which)]
        return remote(place, place, ys.at[pid, source], yr.at[pid, source], y_peer)

    def arrived_z(pid, source):
        place = whole_of[pid].at[piece_rows(pid, source, g)]
        remote(place, place, zs.at[pid, source], zr.at[pid, source], y_peer).wait_recv()

    last = count - 1

    def issue(point):
        for place, plan in enumerate(SENDS):
            @pl.when(s == place)
            def _():
                for pid, dest in plan[point]:
                    z_copy(pid, dest).start()

    def hand_on(pieces):
        for pid, source in pieces:
            arrived_z(pid, source)
            y_copy(pid, source, g).start()

    def serve(point):
        for place, plan in enumerate(FORWARDS):
            @pl.when(s == place)
            def _():
                hand_on(plan[point])

    pl.semaphore_wait(barrier, 3 + count - 1)
    issue(0)

    for i in range(2):
        local[i].wait()
    quad = lambda ref: jnp.concatenate([ref[0], ref[1], ref[0], ref[1]], axis=0)
    raw_forget, raw_input = quad(fgt), quad(inp)
    log_forget = jnp.minimum(raw_forget, 0.0) - jnp.log1p(jnp.exp(-jnp.abs(raw_forget)))
    cum = scan_lanes(log_forget, lambda a, b: a + b, 0.0)
    offset = raw_input - cum
    run = scan_lanes(offset, jnp.maximum, NEG)
    fsum = cum[:, tokens - 1 : tokens]
    top = run[:, tokens - 1 : tokens]
    bmax = fsum + top
    decay = jnp.exp(offset - top)
    offs[...] = offset
    group = 2 * heads
    cols[...] = jnp.transpose(jnp.concatenate([decay[:group], run[:group]], axis=0))

    for i in range(2, 6):
        local[i].wait()
    head_lane = lax.div(lax.broadcasted_iota(jnp.int32, (tokens, heads * DKB), 1), DKB)
    state_of = []
    for h in range(heads):
        column = cols[:, h : h + 1]
        scaled = (ka[:, h * DKA : (h + 1) * DKA].astype(F32) * column).astype(BF16)
        state = lax.dot_general(
            scaled, va[:, h * DV : (h + 1) * DV], TN, preferred_element_type=F32
        )
        bstate[h * DKA : (h + 1) * DKA, :] = state
        state_of.append((h * DKA, DKA, h))
    base_b = heads * DKA
    for h in range(heads):
        column = cols[:, heads + h : heads + h + 1]
        scaled = (kb[...].astype(F32) * column).astype(BF16)
        state = lax.dot_general(
            scaled, vb[:, h * DV : (h + 1) * DV], TN, preferred_element_type=F32
        )
        bstate[base_b + h * DKB : base_b + (h + 1) * DKB, :] = state[h * DKB : (h + 1) * DKB]
        state_of.append((base_b + h * DKB, DKB, heads + h))

    after_peer = (g, jnp.minimum(s + 1, last), t)
    chain = [
        remote(
            st_out.at[pl.ds(start, size)], st_in.at[pl.ds(start, size)],
            cs.at[h], cr.at[h], after_peer,
        )
        for start, size, h in state_of
    ]
    chain_stat = remote(stat_out, stat_in, cs.at[group], cr.at[group], after_peer)
    wide = lambda row: jnp.concatenate([row] * (DV // 128), axis=1)

    def combine_stat():
        before = stat_in[...]
        total = before + fsum
        after = jnp.maximum(total, bmax)
        stat_out[...] = after
        chain_stat.start()
        return jnp.exp(total - after), jnp.exp(jnp.broadcast_to(bmax, total.shape) - after)

    def combine_head(i, keep_old, keep_new):
        start, size, h = state_of[i]
        st_out[start : start + size, :] = (
            wide(keep_old[h : h + 1, :]) * st_in[start : start + size, :].astype(F32)
            + wide(keep_new[h : h + 1, :]) * bstate[start : start + size, :]
        ).astype(BF16)
        chain[i].start()

    @pl.when(s == 0)
    def _():
        st_in[...] = jnp.zeros_like(st_in)
        stat_in[...] = jnp.full_like(stat_in, NEG)
        keeps = combine_stat()
        for i in range(group):
            combine_head(i, *keeps)
        issue(1)

    for copy in local[8:]:
        copy.start()
    for i in range(6, 8):
        local[i].wait()
    causal = lax.broadcasted_iota(jnp.int32, (tokens, tokens), 0) >= lax.broadcasted_iota(
        jnp.int32, (tokens, tokens), 1
    )

    def query_of(h):
        if h < heads:
            return qa[:, h * DKA : (h + 1) * DKA]
        return jnp.where(head_lane == h - heads, qb[...], jnp.zeros_like(qb[...]))

    for h in range(group):
        key = ka[:, h * DKA : (h + 1) * DKA] if h < heads else kb[...]
        value_ref, at = (va, h) if h < heads else (vb, h - heads)
        width = DKA if h < heads else DKB
        scores = lax.dot_general(query_of(h), key, NT, preferred_element_type=F32)
        exponent = jnp.where(causal, offs[h : h + 1, :] - cols[:, group + h : group + h + 1], NEG)
        weights = (scores * width ** (-0.5) * jnp.exp(exponent)).astype(BF16)
        intra[h] = jnp.dot(
            weights, value_ref[:, at * DV : (at + 1) * DV], preferred_element_type=F32
        )

    @pl.when(jnp.logical_and(s > 0, s < last))
    def _():
        chain_stat.wait_recv()
        keeps = combine_stat()
        for i in range(group):
            chain[i].wait_recv()
            combine_head(i, *keeps)
        issue(1)

    @pl.when(s == last)
    def _():
        chain_stat.wait_recv()
        for copy in chain:
            copy.wait_recv()

    serve(0)
    for i in range(8, 10):
        local[i].wait()
    for h in range(group):
        width = DKA if h < heads else DKB
        gate_ref, at = (oga, h) if h < heads else (ogb, h - heads)
        state = (
            st_in[h * DKA : (h + 1) * DKA, :] if h < heads else st_in[base_b:, :]
        )
        entering_max = stat_in[h : h + 1, 0:1]
        own_max = cols[:, group + h : group + h + 1]
        top_max = jnp.maximum(own_max, entering_max)
        carried = jnp.dot(query_of(h), state, preferred_element_type=F32)
        numer = carried * (width ** (-0.5) * jnp.exp(entering_max - top_max)) + intra[
            h
        ] * jnp.exp(own_max - top_max)
        inv = lax.rsqrt(jnp.mean(numer * numer, axis=1, keepdims=True) + EPS)
        gated = numer * inv * jax.nn.sigmoid(gate_ref[:, at * DV : (at + 1) * DV].astype(F32))
        hidden[:, h * DV : (h + 1) * DV] = gated.astype(BF16)

    serve(1)

    for i in range(10, 13):
        local[i].wait()
    chunks1 = proj.shape[0] // chunk1

    def block_rows(chip, core):
        return pl.ds(pl.multiple_of((2 * chip + core) * block, 8), block)

    def d1(j):
        return remote(dsend1.at[j], drecv1.at[j], d1s.at[j], d1r.at[j], core_peer)

    def x1(j):
        return remote(xsend1.at[j], xrecv1.at[j], x1s.at[j], x1r.at[j], x_peer)

    def attn_step(j, carry):
        @pl.when(j < chunks1)
        def _():
            weight = proj[pl.ds(pl.multiple_of(j * chunk1, chunk1), chunk1)]
            part1[...] = lax.dot_general(
                hidden[...], weight.reshape(chunk1, hidden.shape[1]), NT,
                preferred_element_type=F32,
            )
            for role in range(2):
                chip = x if role == 0 else 1 - x
                dsend1[j, role] = part1[block_rows(chip, 1 - c)].astype(BF16)
                keep1[j, role] = part1[block_rows(chip, c)]
            d1(j).start()

        @pl.when(j >= 1)
        def _():
            k = j - 1
            d1(k).wait_recv()
            xsend1[k] = (keep1[k, 1] + drecv1[k, 1].astype(F32)).astype(BF16)
            x1(k).start()
            keep1[k, 0] = keep1[k, 0] + drecv1[k, 0].astype(F32)

        return carry

    lax.fori_loop(0, chunks1 + 1, attn_step, 0)
    issue(2)
    serve(2)
    for j in range(chunks1):
        span = slice(j * chunk1, (j + 1) * chunk1)
        x1(j).wait_recv()
        rsum[:, span] = res[:, span].astype(F32) + keep1[j, 0] + xrecv1[j].astype(F32)
    summed = rsum[...]
    scale = lax.rsqrt(jnp.mean(summed * summed, axis=1, keepdims=True) + EPS)
    mine = block_rows(x, c)
    rows[0, mine] = (summed * scale * gn[...]).astype(BF16)

    def move(kind, src_place, dst_place, chip, core, device):
        return remote(
            rows.at[src_place, block_rows(chip, core)],
            rows.at[dst_place, block_rows(chip, core)],
            ags.at[kind], agr.at[kind], device,
        )

    own_z = move(2, 0, 1, x, c, pair)
    own_x = move(1, 0, 0, x, c, x_peer)
    own_d = move(0, 0, 0, x, c, core_peer)
    own_z.start()
    own_x.start()
    own_d.start()
    issue(3)

    def arrived(kind, place, chip, core):
        move(kind, place, place, chip, core, core_peer).wait_recv()

    serve(3)
    issue(4)
    arrived(1, 0, 1 - x, c)
    fwd_x = move(3, 0, 0, 1 - x, c, core_peer)
    fwd_x.start()
    serve(4)
    arrived(2, 1, x, c)
    fwd_zx = move(5, 1, 1, x, c, x_peer)
    fwd_zd = move(4, 1, 1, x, c, core_peer)
    fwd_zx.start()
    fwd_zd.start()
    issue(5)
    serve(5)

    def take_y(pids):
        for place in range(count):
            @pl.when(place != s)
            def _():
                for pid in pids:
                    y_copy(pid, place, 1 - g).wait_recv()

    for i in range(13, 16):
        local[i].wait()
    take_y(gates)
    arrived(0, 0, x, 1 - c)
    arrived(3, 0, 1 - x, 1 - c)
    act[0] = jnp.dot(rows[0], wg[...], preferred_element_type=F32)
    serve(6)
    arrived(5, 1, 1 - x, c)
    issue(6)
    fwd_xd = move(6, 1, 1, 1 - x, c, core_peer)
    fwd_xd.start()
    serve(7)
    arrived(4, 1, x, 1 - c)
    arrived(6, 1, 1 - x, 1 - c)
    act[1] = jnp.dot(rows[1], wg[...], preferred_element_type=F32)
    serve(8)
    take_y(ups)

    def up_step(p, carry):
        gate = act[p]
        up = jnp.dot(rows[p], wu[...], preferred_element_type=F32)
        start = pl.multiple_of(p * tokens, tokens)
        inner[pl.ds(start, tokens), :] = (gate / (1.0 + jnp.exp(-gate)) * up).astype(BF16)
        return carry

    lax.fori_loop(0, 2, up_step, 0)
    issue(7)

    rounds = count * SUBS
    chunks2 = 2 * rounds

    def look(table, k):
        value = jnp.int32(table[0])
        for i, entry in enumerate(table[1:], 1):
            value = jnp.where(k == i, entry, value)
        return value

    low = s < count // 2

    def place_of(p):
        is_y = jnp.logical_or(
            jnp.logical_and(p > 0, lax.rem(p, 2) == 0), p == chunks2 - 1
        )
        r = jnp.where(
            p == chunks2 - 1, rounds - 1,
            jnp.where(is_y, lax.div(p, 2) - 1, lax.div(p + 1, 2)),
        )
        r = jnp.maximum(r, 0)
        b, sub = (
            jnp.where(low, *(look([pick[i] for pick in order], r) for order in ROUNDS))
            for i in range(2)
        )
        which = jnp.where(is_y, 1 - g, g)
        return b, sub, which, is_y, r

    def down_rows(p):
        b, sub, which, _, _ = place_of(p)
        return b * depth + which * part_rows + sub * sub_rows

    def d2(k):
        return remote(dsend2.at[k], drecv2.at[k], d2s.at[k], d2r.at[k], core_peer)

    def x2(k):
        return remote(xsend2.at[k], xrecv2.at[k], x2s.at[k], x2r.at[k], x_peer)

    def z2(k):
        return remote(zsend2.at[k], zrecv2.at[k], z2s.at[k], z2r.at[k], pair)

    lag_d = chunks2

    def down_step(p, carry):
        @pl.when(p < chunks2)
        def _():
            b, sub, _, is_y, r = place_of(p)
            start = pl.multiple_of(down_rows(p), sub_rows)
            spot = wd.at[pl.ds(start, sub_rows)]
            pid = 2 * SUBS + sub
            y_both = remote(spot, spot, ys.at[pid, b], yr.at[pid, b], y_peer)

            for place, plan in enumerate(LATE):
                for k, pieces in enumerate(plan):
                    if pieces:
                        now = jnp.logical_and(s == place, r == k)

                        @pl.when(jnp.logical_and(now, jnp.logical_not(is_y)))
                        def _():
                            hand_on(pieces)

            @pl.when(jnp.logical_and(b != s, is_y))
            def _():
                y_both.wait_recv()

            part2[...] = lax.dot_general(
                inner[...], wd[pl.ds(start, sub_rows), :], NT, preferred_element_type=F32
            )
            ring = lax.rem(p, RING)
            for place in range(2):
                for role in range(2):
                    chip = x if role == 0 else 1 - x
                    send = pl.multiple_of(place * tokens + (2 * chip + 1 - c) * block, 8)
                    hold = pl.multiple_of(place * tokens + (2 * chip + c) * block, 8)
                    dsend2[p, 2 * place + role] = part2[pl.ds(send, block)].astype(BF16)
                    keep2[ring, 2 * place + role] = part2[pl.ds(hold, block)]
            d2(p).start()

        @pl.when(jnp.logical_and(p >= LAG_B, p < chunks2 + LAG_B))
        def _():
            k = p - LAG_B
            ring = lax.rem(k, RING)
            d2(k).wait_recv()
            for place in range(2):
                xsend2[k, place] = (
                    keep2[ring, 2 * place + 1] + drecv2[k, 2 * place + 1].astype(F32)
                ).astype(BF16)
            x2(k).start()
            for place in range(2):
                keep2[ring, 2 * place] = keep2[ring, 2 * place] + drecv2[
                    k, 2 * place
                ].astype(F32)

        @pl.when(jnp.logical_and(p >= LAG_C, p < chunks2 + LAG_C))
        def _():
            k = p - LAG_C
            ring = lax.rem(k, RING)
            x2(k).wait_recv()
            zsend2[k] = (keep2[ring, 2] + xrecv2[k, 1].astype(F32)).astype(BF16)
            z2(k).start()
            span = pl.ds(pl.multiple_of(down_rows(k), sub_rows), sub_rows)
            rsum[:, span] = rsum[:, span] + keep2[ring, 0] + xrecv2[k, 0].astype(F32)

        @pl.when(p >= lag_d)
        def _():
            k = p - lag_d
            z2(k).wait_recv()
            span = pl.ds(pl.multiple_of(down_rows(k), sub_rows), sub_rows)
            out_ref[:, span] = (rsum[:, span] + zrecv2[k].astype(F32)).astype(BF16)

        return carry

    lax.fori_loop(0, chunks2 + lag_d, down_step, 0)

    for pid in range(3 * SUBS):
        for dest in range(count):
            @pl.when(dest != s)
            def _():
                z_copy(pid, dest).wait_send()
                y_copy(pid, dest, g).wait_send()

    @pl.when(s < last)
    def _():
        chain_stat.wait_send()
        for copy in chain:
            copy.wait_send()

    for copy in (own_z, own_x, own_d, fwd_x, fwd_zx, fwd_zd, fwd_xd):
        copy.wait_send()
    for j in range(chunks1):
        d1(j).wait_send()
        x1(j).wait_send()

    def drain(k, carry):
        d2(k).wait_send()
        x2(k).wait_send()
        z2(k).wait_send()
        return carry

    lax.fori_loop(0, chunks2, drain, 0)


def fused(*args):
    query_a, _, _, _, _ = args[:5]
    resid, w_gate = args[10], args[13]
    count = lax.axis_size("sp")
    tokens = query_a.shape[0]
    heads = query_a.shape[1] // DKA
    depth, units = w_gate.shape
    half = units // 2
    block, width = resid.shape
    chunk1 = width // 4
    chunk2 = depth // 2 // SUBS
    chunks1, chunks2 = width // chunk1, width // chunk2
    group = 2 * heads
    state_rows = heads * (DKA + DKB)
    sizes = (count, tokens, heads, depth, half, block, chunk1, chunk2)
    args = list(args)
    args[12] = args[12].reshape(1, width)
    vmem = lambda *shape, kind=BF16: pltpu.VMEM(shape, kind)
    dma = pltpu.SemaphoreType.DMA
    pieces = (3 * SUBS, count)
    copies = [args[i] for i in (0, 1, 2, 3, 4, 5, 6, 7, 8, 9, 10, 11, 12)]
    scratch = [pltpu.VMEM(a.shape, a.dtype) for a in copies]
    scratch += [vmem(width, half), vmem(width, half), vmem(width, half)]
    scratch += [
        vmem(tokens, 2 * group, kind=F32),
        vmem(2 * group, tokens, kind=F32),
        vmem(state_rows, DV, kind=F32),
        vmem(state_rows, DV),
        vmem(state_rows, DV),
        vmem(2 * group, 128, kind=F32),
        vmem(2 * group, 128, kind=F32),
        vmem(group, tokens, DV, kind=F32),
        vmem(tokens, group * DV),
        vmem(tokens, chunk1, kind=F32),
        vmem(chunks1, 2, block, chunk1, kind=F32),
        vmem(chunks1, 2, block, chunk1),
        vmem(chunks1, 2, block, chunk1),
        vmem(chunks1, block, chunk1),
        vmem(chunks1, block, chunk1),
        vmem(block, width, kind=F32),
        vmem(2, tokens, width),
        vmem(2, tokens, half, kind=F32),
        vmem(2 * tokens, half),
        vmem(2 * tokens, chunk2, kind=F32),
        vmem(RING, 4, block, chunk2, kind=F32),
        vmem(chunks2, 4, block, chunk2),
        vmem(chunks2, 4, block, chunk2),
        vmem(chunks2, 2, block, chunk2),
        vmem(chunks2, 2, block, chunk2),
        vmem(chunks2, block, chunk2),
        vmem(chunks2, block, chunk2),
    ]
    scratch += [dma((16,)), dma(pieces), dma(pieces), dma(pieces), dma(pieces), dma((group + 1,)), dma((group + 1,))]
    scratch += [dma((chunks1,))] * 4 + [dma((7,))] * 2 + [dma((chunks2,))] * 6
    return pl.pallas_call(
        functools.partial(fused_body, sizes),
        out_shape=jax.ShapeDtypeStruct(resid.shape, BF16),
        in_specs=[pl.BlockSpec(memory_space=pl.ANY)] * len(args),
        out_specs=pl.BlockSpec(memory_space=pltpu.VMEM),
        scratch_shapes=scratch,
        compiler_params=pltpu.CompilerParams(
            collective_id=0, has_side_effects=True, vmem_limit_bytes=VMEM_BYTES
        ),
    )(*args)


def layer(*args):
    return local(*args)


def solution(mesh):
    few = mesh.shape["sp"] == 4 and mesh.shape["tp"] == 4
    return jax.shard_map(
        fused if few else layer,
        mesh=mesh,
        in_specs=(
            P(("grp", "sp"), "tp"),
            P(("grp", "sp"), "tp"),
            P(("grp", "sp"), "tp"),
            P(("grp", "sp"), "tp"),
            P(("grp", "sp"), "tp"),
            P(("grp", "sp"), "tp"),
            P(("grp", "sp"), "tp"),
            P(("grp", "sp"), "tp"),
            P(None, "tp", ("grp", "sp")),
            P(None, "tp", ("grp", "sp")),
            P(("grp", "sp", "tp"), None),
            P(None, None, "tp"),
            P(),
            P("sp", "tp"),
            P("sp", "tp"),
            P("sp", "tp"),
        ),
        out_specs=P(("grp", "sp", "tp"), None),
        check_vma=False,
    )
```
